256 devices in a mesh: grp: 2 (over y), sp: 32 (over z, core), tp: 4 (over x).
Axes of the slice: x: 4, y: 2, z: 16, core: 2. Of those that a mesh axis runs over, the one named last changes fastest.
The devices are a block of a 4x16x16 slice.
Arguments:
- resid: bfloat16 [12288, 2048], P(('grp', 'sp', 'tp')), parts along dimension 0, may hold values from -6 to 6
- queries: bfloat16 [12288, 1024], P(('grp', 'sp'), 'tp'), parts along dimension 0, may hold values from -64 to 64
- keys: bfloat16 [12288, 256], P(('grp', 'sp'), 'tp'), parts along dimension 0, may hold values from -64 to 64
- values: bfloat16 [12288, 256], P(('grp', 'sp'), 'tp'), parts along dimension 0, may hold values from -6 to 6
- doc_ids: int32 [12288], P(('grp', 'sp')), parts along dimension 0, may hold values from 0 to 15, never falling along the last dimension, each value on 1 to 768 neighbouring positions
- sink_logits: float32 [16], P('tp'), may hold values from 2 to 6
- out_proj: bfloat16 [1024, 2048], P('tp'), may hold values from -1.5 to 1.5
- norm1_gain: float32 [2048], replicated, may hold values from 0.1 to 1.9
- norm1_bias: float32 [2048], replicated, may hold values from -1.8 to 1.8
- route_ids: int32 [12288, 2], P(('grp', 'sp', 'tp')), parts along dimension 0, may hold values from 0 to 31, all different within a row; in each aligned block of 48 rows (0 to 47, 48 to 95, ...) at most 3 rows name the same one
- route_weights: float32 [12288, 2], P(('grp', 'sp', 'tp')), parts along dimension 0, may hold values from 0.25 to 1
- expert_gate: bfloat16 [32, 2048, 3072], P('sp', None, 'tp'), may hold values from -0.125 to 0.125
- expert_up: bfloat16 [32, 2048, 3072], P('sp', None, 'tp'), may hold values from -0.125 to 0.125
- expert_down: bfloat16 [32, 3072, 2048], P('sp', 'tp'), may hold values from -0.109375 to 0.109375
- norm2_gain: float32 [2048], replicated, may hold values from 0.1 to 1.9
- norm2_bias: float32 [2048], replicated, may hold values from -1.8 to 1.8
Outputs:
- mixed: bfloat16 [12288, 2048], P(('grp', 'sp', 'tp')), parts along dimension 0
The draws below stay inside these ranges and needn't reach their ends.
There are 2 independent parts, one for each index of `grp`. The reference program is written for one: setup_inputs(seed, part) draws one part's arguments, and reference() takes and returns one part's arrays. A program takes and returns all parts, laid end to end along the dimension named above; an argument that names none is the same for every part. Nothing has to cross between parts.
Inputs may be any that keep to these rules, and one draw needn't show every extreme that they name: `route_ids`: among the rows of one device (aligned blocks of 48 tokens) no expert is named more than 3 times, a bound that some block reaches; a token's 2 experts differ.
All inputs are finite; a program needn't handle non-finite values.
Results may differ from the reference program's by a relative error of at most 0.012.
Values may be sent and summed in bfloat16 or wider, within the bound.
No kernel may reach another device: no remote copies, remote signals or barrier semaphores. Data moves between devices by JAX's collectives and lax.ppermute only.
A program may use at most 64 MiB of HBM per device.

```python
import math
import jax
import jax.numpy as jnp
import numpy as np
from jax import lax

D = 2048
HEADS = 16
KV_HEADS = 4
HEAD_DIM = 64
ATT_WIDTH = 1024
FF = 3072
TOPK = 2
WINDOW = 128
TOK_DEV = 192
TOK_SUB = 48
TOKENS = 6144
EXPERTS = 32
CAP = 3
DOCS = 16
DOC_MOST = 768
N_TP = 4


def draw_keys(key, part):
    noise = jnp.clip(jax.random.normal(jax.random.fold_in(key, 1), (TOKENS, KV_HEADS, HEAD_DIM), jnp.float32), -6.0, 6.0)
    return noise.reshape(TOKENS, KV_HEADS * HEAD_DIM).astype(jnp.bfloat16)


def draw_queries(key, part):
    noise = jnp.clip(jax.random.normal(jax.random.fold_in(key, 2), (TOKENS, HEADS, HEAD_DIM), jnp.float32), -6.0, 6.0)
    return noise.reshape(TOKENS, HEADS * HEAD_DIM).astype(jnp.bfloat16)


def block_levels(key, dims, cuts, smallest, high):
    gain, own = 1.0, jax.random.fold_in(key, 6)
    for dim, parts in cuts:
        draws = jnp.exp(jax.random.uniform(jax.random.fold_in(own, dim), (parts,), jnp.float32, smallest / len(cuts), high / len(cuts)))
        gain = gain * jnp.repeat(draws, dims[dim] // parts).reshape([-1 if axis == dim else 1 for axis in range(len(dims))])
    return gain


def profile(number_of, total, most, slope):
    weights = [(1 << 20) // math.isqrt(standing ** slope) + 1 for standing in range(2, number_of + 1)]
    surplus, holding = total - most - (number_of - 1), [1] * (number_of - 1)
    while surplus > 0:
        free = [i for i in range(number_of - 1) if holding[i] < most]
        whole, budget = sum([weights[i] for i in free]), surplus
        for i in free:
            extra = min(most - holding[i], max(1, budget * weights[i] // whole), surplus)
            holding[i] = holding[i] + extra
            surplus = surplus - extra
    return np.array([most] + holding)


def uneven(rng, amount, total, most, lean):
    if amount == 2:
        one = jax.random.randint(rng, (), max(1, total - most), min(most, total - 1) + 1)
        return jnp.stack([one, total - one])
    lengths = jnp.asarray(profile(amount, total, most, lean), jnp.int32)
    pairs = (amount - 1) // 2
    source_of, sink = lengths[1:1 + 2 * pairs:2], lengths[2:2 + 2 * pairs:2]
    room = jnp.minimum(source_of - 1, most - sink)
    moved = jax.random.randint(jax.random.fold_in(rng, 1), (pairs,), 0, 1 << 20) % (room + 1)
    lengths = lengths.at[1:1 + 2 * pairs:2].set(source_of - moved).at[2:2 + 2 * pairs:2].set(sink + moved)
    return lengths[jax.random.permutation(jax.random.fold_in(rng, 2), amount)]


def assign_block(rng, own, number, rows, count, top, most, skew):
    sequence = jax.random.permutation(rng, count)
    packed, usual = load_shares(count, rows * top, most, skew, True), load_shares(count, rows * top, most, skew, False)
    places = jnp.arange(count)

    def named(sizes, rotation):
        used = int((sizes > 0).sum())
        fixed = max(1, used // 4)
        moved = fixed + (places - fixed + rotation * (used - fixed)) % max(1, count - fixed)
        return jnp.zeros((count,), jnp.int32).at[sequence[jnp.where(places < fixed, places, moved)]].set(jnp.asarray(sizes, jnp.int32))

    sizes = jnp.where(number % 4 == 0, named(packed, number // 4), named(usual, number - number // 4 - 1))
    mixed = jax.random.permutation(jax.random.fold_in(own, 3), count)
    donor, sink = mixed[0:count // 2 * 2:2], mixed[1:count // 2 * 2:2]
    room = jnp.minimum(sizes[donor] - 1, most - sizes[sink]) // 2
    room = jnp.where((donor == sequence[0]) | (sink == sequence[0]) | (sizes[sink] == 0), 0, jnp.maximum(room, 0))
    moved = jax.random.randint(jax.random.fold_in(own, 4), (count // 2,), 0, 1 << 20) % (room + 1)
    sizes = sizes.at[donor].add(-moved).at[sink].add(moved)
    labels = jnp.searchsorted(jnp.cumsum(sizes), jnp.arange(rows * top), side="right").astype(jnp.int32)
    grid = labels.reshape(top, rows).T
    grid = grid[jax.random.permutation(jax.random.fold_in(own, 1), rows)]
    rotation = jax.random.randint(jax.random.fold_in(own, 2), (rows, 1), 0, top)
    return jnp.take_along_axis(grid, (jnp.arange(top)[None, :] + rotation) % top, axis=1)


def load_shares(amount, total, limit, skew, full):
    weights = [(1 << 20) // math.isqrt(grade ** skew) + 1 for grade in range(1, amount + 1)]
    largest = limit if full else min(limit, max(-(-total // amount), total * weights[0] // sum(weights)))
    least = 1 if total - largest >= amount - 1 else 0
    given, rest = [largest] + [least] * (amount - 1), total - largest - least * (amount - 1)
    while rest > 0:
        free = [i for i in range(1, amount) if given[i] < largest] or [i for i in range(1, amount) if given[i] < limit]
        mass, budget = sum([weights[i] for i in free]), rest
        for i in free:
            extra = min(limit - given[i], max(1, budget * weights[i] // mass), rest)
            given[i] = given[i] + extra
            rest = rest - extra
    return np.array(given)


def normal_values(own_key, extent, spread, most, shards=(), held_as=jnp.bfloat16):
    values = jax.random.normal(own_key, extent, jnp.float32) * spread
    if len(shards) > 0:
        values = block_levels(own_key, extent, shards, -0.22, 0.18) * values
    return jnp.clip(values, min=-most, max=most).astype(held_as)


def setup_inputs(seed: int = 0, part: int = 0) -> dict:
    seeds = jax.random.split(jax.random.key(seed), 17)
    part_keys = jax.random.split(jax.random.fold_in(seeds[16], part), 17)
    resid = normal_values(part_keys[0], (TOKENS, D), 1.0, 6.0, ((0, 128),))
    queries = draw_queries(jax.random.fold_in(jax.random.fold_in(seeds[16], part), 71), part)
    keys = draw_keys(jax.random.fold_in(jax.random.fold_in(seeds[16], part), 71), part)
    values = normal_values(part_keys[3], (TOKENS, KV_HEADS * HEAD_DIM), 1.0, 6.0, ((0, 32), (1, 4)))
    doc_ids = jnp.searchsorted(jnp.cumsum(uneven(part_keys[4], DOCS, TOKENS, DOC_MOST, 2)), jnp.arange(TOKENS), side="right").astype(jnp.int32)
    sink_logits = jnp.clip(2.0 + 4.0 * jax.random.uniform(seeds[5], (HEADS,), jnp.float32) ** block_levels(seeds[5], (HEADS,), ((0, 4),), -0.2, 0.2), 2.0, 6.0)
    out_proj = normal_values(seeds[6], (ATT_WIDTH, D), (HEAD_DIM // 4) ** -0.5, 1.5, ((0, 4),))
    norm1_gain = jnp.clip(1.0 + 0.18 * jax.random.normal(seeds[7], (D,), jnp.float32), 0.1, 1.9)
    norm1_bias = normal_values(seeds[8], (D,), 0.3, 1.8, (), jnp.float32)
    route_ids_keys = jax.random.split(jax.random.fold_in(part_keys[9], 1), TOKENS // TOK_SUB)
    route_ids_turns = jax.random.permutation(jax.random.fold_in(part_keys[9], 3), TOKENS // TOK_SUB)
    route_ids = jax.vmap(lambda own, number: assign_block(jax.random.fold_in(part_keys[9], 2), own, number, TOK_SUB, EXPERTS, TOPK, CAP, 1))(route_ids_keys, route_ids_turns).reshape((TOKENS, TOPK))
    route_weights = jnp.clip(0.25 + 0.75 * jax.random.uniform(part_keys[10], (TOKENS, TOPK), jnp.float32) ** block_levels(part_keys[10], (TOKENS, TOPK), ((0, 128),), -0.2, 0.2), 0.25, 1.0)
    expert_gate = normal_values(seeds[11], (EXPERTS, D, FF), D ** -0.5, 0.125, ((0, 32), (2, 4)))
    expert_up = normal_values(seeds[12], (EXPERTS, D, FF), D ** -0.5, 0.125, ((0, 32), (2, 4)))
    expert_down = normal_values(seeds[13], (EXPERTS, FF, D), FF ** -0.5, 0.109375, ((0, 32), (1, 4)))
    norm2_gain = jnp.clip(1.0 + 0.18 * jax.random.normal(seeds[14], (D,), jnp.float32), 0.1, 1.9)
    norm2_bias = normal_values(seeds[15], (D,), 0.3, 1.8, (), jnp.float32)
    return {"resid": resid, "queries": queries, "keys": keys, "values": values, "doc_ids": doc_ids, "sink_logits": sink_logits, "out_proj": out_proj, "norm1_gain": norm1_gain, "norm1_bias": norm1_bias, "route_ids": route_ids, "route_weights": route_weights, "expert_gate": expert_gate, "expert_up": expert_up, "expert_down": expert_down, "norm2_gain": norm2_gain, "norm2_bias": norm2_bias}


norm_epsilon = 1e-05
residual_scale = 1.4142135623730951
masked_score = -1e+30

def layer_norm(values, gain_vec, bias_vec):
    mean_val = lax.optimization_barrier(jnp.mean(values, -1, keepdims=True))
    centred = values - mean_val
    variance = lax.optimization_barrier(jnp.mean(centred * centred, -1, keepdims=True))
    return centred * lax.rsqrt(variance + norm_epsilon) * gain_vec + bias_vec

def attention(queries, keys, values, doc_ids, sink_logits):
    groups = HEADS // KV_HEADS
    block = TOK_DEV
    nblocks = TOKENS // block
    reach = block + 2 * WINDOW
    pad_keys = jnp.pad(keys.reshape(TOKENS, KV_HEADS, HEAD_DIM), ((WINDOW, WINDOW), (0, 0), (0, 0)))
    pad_values = jnp.pad(values.reshape(TOKENS, KV_HEADS, HEAD_DIM), ((WINDOW, WINDOW), (0, 0), (0, 0)))
    pad_docs = jnp.pad(doc_ids.astype(jnp.int32), (WINDOW, WINDOW))
    sink_table = sink_logits.astype(jnp.float32).reshape(KV_HEADS, groups, 1, 1)

    def one_block(index):
        start = index * block
        query_blk = lax.dynamic_slice_in_dim(queries, start, block, 0).reshape(block, KV_HEADS, groups, HEAD_DIM)
        key_blk = lax.dynamic_slice_in_dim(pad_keys, start, reach, 0)
        value_blk = lax.dynamic_slice_in_dim(pad_values, start, reach, 0)
        query_docs = lax.dynamic_slice_in_dim(doc_ids.astype(jnp.int32), start, block, 0)
        key_docs = lax.dynamic_slice_in_dim(pad_docs, start, reach, 0)
        query_pos = start + jnp.arange(block, dtype=jnp.int32)
        key_pos = start - WINDOW + jnp.arange(reach, dtype=jnp.int32)
        allowed = (key_pos[None, :] >= 0) & (key_pos[None, :] < TOKENS)
        allowed = allowed & (jnp.abs(query_pos[:, None] - key_pos[None, :]) <= WINDOW)
        allowed = allowed & (query_docs[:, None] == key_docs[None, :])
        scores = jnp.einsum('qkgd,jkd->kgqj', query_blk.astype(jnp.float32), key_blk.astype(jnp.float32))
        scores = jnp.where(allowed, scores * HEAD_DIM ** (-0.5), masked_score)
        top_score = jnp.maximum(lax.optimization_barrier(jnp.max(scores, -1, keepdims=True)), sink_table)
        raised = jnp.where(allowed, jnp.exp(scores - top_score), 0.0)
        denominator = jnp.exp(sink_table - top_score) + lax.optimization_barrier(jnp.sum(raised, -1, keepdims=True))
        weights = (raised / denominator).astype(jnp.bfloat16)
        result = jnp.einsum('kgqj,jkd->qkgd', weights.astype(jnp.float32), value_blk.astype(jnp.float32))
        return result.astype(jnp.bfloat16).reshape(block, HEADS * HEAD_DIM)
    blocks = lax.map(one_block, jnp.arange(nblocks, dtype=jnp.int32))
    return blocks.reshape(TOKENS, HEADS * HEAD_DIM)

def experts_part(normed, route_ids, route_weights, expert_gate, expert_up, expert_down):
    nblocks = TOKENS // TOK_SUB
    slot_count = nblocks * CAP
    flat_ids = route_ids.reshape(nblocks, TOK_SUB * TOPK).astype(jnp.int32)
    one_hot = (flat_ids[:, :, None] == jnp.arange(EXPERTS, dtype=jnp.int32)[None, None, :]).astype(jnp.int32)
    ranks = (jnp.cumsum(one_hot, axis=1) - 1).astype(jnp.int32)
    slot_rank = lax.optimization_barrier(jnp.sum(ranks * one_hot, axis=-1)).astype(jnp.int32)
    block_ids = jnp.arange(nblocks, dtype=jnp.int32)[:, None]
    targets = (flat_ids * slot_count + block_ids * CAP + slot_rank).reshape(-1).astype(jnp.int32)
    owners = (block_ids * TOK_SUB + jnp.arange(TOK_SUB * TOPK, dtype=jnp.int32)[None, :] // TOPK).reshape(-1).astype(jnp.int32)
    token_table = jnp.full((EXPERTS * slot_count,), TOKENS, jnp.int32).at[targets].set(owners).reshape(EXPERTS, slot_count)
    weight_table = jnp.zeros((EXPERTS * slot_count,), jnp.float32).at[targets].set(route_weights.reshape(-1).astype(jnp.float32)).reshape(EXPERTS, slot_count)
    padded = jnp.concatenate([normed, jnp.zeros((1, D), normed.dtype)], 0)
    hidden_cols = FF // N_TP

    def one_expert(total, inputs):
        gate_weight, up_weight, down_weight, token_rows, row_weights = inputs
        row_block = jnp.take(padded, token_rows, axis=0)
        gate_act = jnp.dot(row_block, gate_weight, preferred_element_type=jnp.float32)
        up_act = jnp.dot(row_block, up_weight, preferred_element_type=jnp.float32)
        hidden = (jax.nn.silu(gate_act) * up_act).astype(jnp.bfloat16)
        summed = jnp.zeros((slot_count, D), jnp.float32)
        for member in range(N_TP):
            piece_out = jnp.dot(hidden[:, member * hidden_cols:(member + 1) * hidden_cols], down_weight[member * hidden_cols:(member + 1) * hidden_cols], preferred_element_type=jnp.float32)
            summed = summed + lax.optimization_barrier(piece_out.astype(jnp.bfloat16)).astype(jnp.float32)
        expert_out = lax.optimization_barrier(summed.astype(jnp.bfloat16)).astype(jnp.float32)
        return (total.at[token_rows].add(row_weights[:, None] * expert_out), None)
    total, _ = lax.scan(one_expert, jnp.zeros((TOKENS + 1, D), jnp.float32), (expert_gate, expert_up, expert_down, token_table, weight_table))
    return total[:TOKENS]

def reference(resid, queries, keys, values, doc_ids, sink_logits, out_proj, norm1_gain, norm1_bias, route_ids, route_weights, expert_gate, expert_up, expert_down, norm2_gain, norm2_bias):
    attended = attention(queries, keys, values, doc_ids, sink_logits)
    head_cols = ATT_WIDTH // N_TP
    projected = jnp.zeros((TOKENS, D), jnp.float32)
    for member in range(N_TP):
        piece_out = jnp.dot(attended[:, member * head_cols:(member + 1) * head_cols], out_proj[member * head_cols:(member + 1) * head_cols], preferred_element_type=jnp.float32)
        projected = projected + lax.optimization_barrier(piece_out.astype(jnp.bfloat16)).astype(jnp.float32)
    projected = lax.optimization_barrier(projected.astype(jnp.bfloat16)).astype(jnp.float32)
    pre_norm = residual_scale * resid.astype(jnp.float32) + projected
    normed = layer_norm(pre_norm, norm1_gain, norm1_bias).astype(jnp.bfloat16)
    moe_sum = experts_part(normed, route_ids, route_weights, expert_gate, expert_up, expert_down)
    pre_final = residual_scale * normed.astype(jnp.float32) + moe_sum
    return layer_norm(pre_final, norm2_gain, norm2_bias).astype(jnp.bfloat16)
```

```python
import functools

import jax
import jax.numpy as jnp
from jax import lax
from jax.experimental import pallas as pl
from jax.experimental.pallas import tpu as pltpu
from jax.sharding import PartitionSpec as P

HEAD_DIM = 64
WINDOW = 128
LANES = 128
NORM_EPSILON = 1e-05
RESIDUAL_SCALE = 1.4142135623730951
MASKED = -1e30
F32 = jnp.float32
BF16 = jnp.bfloat16


VMEM = pl.BlockSpec(memory_space=pltpu.VMEM)
ANY = pl.BlockSpec(memory_space=pl.ANY)


def mm(a, b):
    return jnp.dot(a, b, preferred_element_type=F32)


def mm_nt(a, b):
    return lax.dot_general(a, b, (((1,), (1,)), ((), ())), preferred_element_type=F32)


def call(body, out_shapes, *args, name, flops, specs=None, scratch=(), vmem=None):
    size = sum(a.size * a.dtype.itemsize for a in args)
    size += sum(s.size * s.dtype.itemsize for s in out_shapes)
    return pl.pallas_call(
        body,
        out_shape=out_shapes,
        in_specs=specs or [VMEM] * len(args),
        out_specs=[VMEM] * len(out_shapes),
        scratch_shapes=list(scratch),
        compiler_params=pltpu.CompilerParams(vmem_limit_bytes=vmem),
        cost_estimate=pl.CostEstimate(flops=flops, bytes_accessed=size, transcendentals=0),
        name=name,
    )(*args)


def shape(dims, dtype):
    return jax.ShapeDtypeStruct(dims, dtype)


def layer_norm(values, gain, bias):
    centred = values - jnp.mean(values, -1, keepdims=True)
    variance = jnp.mean(centred * centred, -1, keepdims=True)
    return centred * lax.rsqrt(variance + NORM_EPSILON) * gain + bias


def pack_body(keys_ref, values_ref, docs_ref, head_ref, tail_ref):
    tokens = keys_ref.shape[1]
    docs = (docs_ref[...].astype(F32) + 1.0).astype(BF16)
    for ref, lo in ((head_ref, 0), (tail_ref, tokens - WINDOW)):
        cols = slice(lo, lo + WINDOW)
        ref[0:HEAD_DIM, :] = keys_ref[:, cols]
        ref[HEAD_DIM : 2 * HEAD_DIM, :] = values_ref[:, cols]
        ref[2 * HEAD_DIM :, :] = jnp.broadcast_to(docs[:, cols], (16, WINDOW))


def attention_body(
    sink_ref, query_ref, keys_ref, values_ref, docs_ref, prev_ref, next_ref, proj_ref, out_ref, att_ref
):
    tokens = query_ref.shape[0]
    heads = query_ref.shape[1] // HEAD_DIM
    own_docs = docs_ref[...].astype(F32) + 1.0
    query_docs = jnp.broadcast_to(own_docs, (LANES, tokens)).T[:, 0:1]
    row = lax.broadcasted_iota(jnp.int32, (tokens, 1), 0)
    blocks = []
    for key, value, docs, first in (
        (prev_ref[0:HEAD_DIM, :], prev_ref[HEAD_DIM : 2 * HEAD_DIM, :], None, -WINDOW),
        (keys_ref[...], values_ref[...], own_docs, 0),
        (next_ref[0:HEAD_DIM, :], next_ref[HEAD_DIM : 2 * HEAD_DIM, :], None, tokens),
    ):
        if docs is None:
            ref = prev_ref if first < 0 else next_ref
            docs = ref[2 * HEAD_DIM :, :].astype(F32)[0:1, :]
        width = key.shape[1]
        place = first + lax.broadcasted_iota(jnp.int32, (1, width), 1)
        allowed = (jnp.abs(row - place) <= WINDOW) & (query_docs == docs)
        blocks.append((key, value, allowed))
    for h in range(heads):
        cols = slice(h * HEAD_DIM, (h + 1) * HEAD_DIM)
        query = query_ref[:, cols]
        sink = sink_ref[0, h]
        scores = [
            jnp.where(allowed, mm(query, key) * HEAD_DIM ** (-0.5), MASKED)
            for key, _, allowed in blocks
        ]
        top = functools.reduce(jnp.maximum, [jnp.max(s, -1, keepdims=True) for s in scores])
        top = jnp.maximum(top, sink)
        raised = [
            jnp.where(allowed, jnp.exp(s - top), 0.0) for s, (_, _, allowed) in zip(scores, blocks)
        ]
        total = jnp.exp(sink - top) + sum(jnp.sum(r, -1, keepdims=True) for r in raised)
        scale = 1.0 / total
        result = sum(
            mm_nt((r * scale).astype(BF16), value) for r, (_, value, _) in zip(raised, blocks)
        )
        att_ref[:, cols] = result.astype(BF16)
    out_ref[...] = mm(att_ref[...], proj_ref[...]).astype(BF16)


def routing_rows(ids, experts, tokens):
    expert = lax.broadcasted_iota(jnp.int32, (experts, tokens), 0)
    named = jnp.zeros((experts, tokens), F32)
    for k in range(ids.shape[0]):
        named += (ids[k : k + 1, :] == expert).astype(F32)
    before = lax.broadcasted_iota(jnp.int32, (tokens, tokens), 0) < lax.broadcasted_iota(
        jnp.int32, (tokens, tokens), 1
    )
    rank = mm(named.astype(BF16), before.astype(BF16))
    return named, rank


def dispatch_body(
    experts, parts_ref, resid_ref, gain_ref, bias_ref, ids_ref, normed_ref, sent_ref, wide_ref
):
    tokens, width = resid_ref.shape
    tiles = width // LANES
    capacity = ids_ref.shape[0] * tokens // experts
    projected = sum(parts_ref[i].astype(F32) for i in range(parts_ref.shape[0]))
    pre_norm = RESIDUAL_SCALE * resid_ref[...].astype(F32) + projected.astype(BF16).astype(F32)
    normed = layer_norm(pre_norm, gain_ref[...], bias_ref[...]).astype(BF16)
    normed_ref[...] = normed
    named, rank = routing_rows(ids_ref[...], experts, tokens)
    for j in range(capacity):
        pick = jnp.where((named > 0.5) & (jnp.abs(rank - j) < 0.5), 1.0, 0.0).astype(BF16)
        rows = mm(pick, normed)
        for c in range(tiles):
            wide_ref[pl.ds(j * tiles + c, experts, stride=capacity * tiles), :] = rows[
                :, c * LANES : (c + 1) * LANES
            ]
    sent_ref[...] = wide_ref[...].astype(BF16)


def expert_body(*refs):
    row_refs, refs = refs[:4], refs[4:]
    gate_hbm, up_hbm, down_hbm, *refs = refs
    out_refs, refs = refs[:4], refs[4:]
    gate, up, down, lhs, wide, gate_sem, up_sem, down_sem = refs
    chunks = gate_sem.shape[0]
    width, hidden = gate.shape
    tiles = width // LANES
    rows = row_refs[0].shape[0] // tiles
    step = width // chunks
    gate_copy = [
        pltpu.make_async_copy(
            gate_hbm.at[pl.ds(i * step, step)], gate.at[pl.ds(i * step, step)], gate_sem.at[i]
        )
        for i in range(chunks)
    ]
    up_copy = [
        pltpu.make_async_copy(
            up_hbm.at[pl.ds(i * step, step)], up.at[pl.ds(i * step, step)], up_sem.at[i]
        )
        for i in range(chunks)
    ]
    down_copy = [
        pltpu.make_async_copy(
            down_hbm.at[:, pl.ds(i * step, step)], down.at[:, pl.ds(i * step, step)], down_sem.at[i]
        )
        for i in range(chunks)
    ]
    for a, b in zip(gate_copy, up_copy):
        a.start()
        b.start()
    for a in down_copy:
        a.start()
    for b, ref in enumerate(row_refs):
        wide[b] = ref[...].astype(F32)
        for c in range(tiles):
            lhs[b * rows : (b + 1) * rows, c * LANES : (c + 1) * LANES] = wide.at[b][
                pl.ds(c, rows, stride=tiles), :
            ].astype(BF16)
    gate_act, up_act = 0.0, 0.0
    for i in range(chunks):
        cols = slice(i * step, (i + 1) * step)
        gate_copy[i].wait()
        gate_act += mm(lhs[:, cols], gate[cols, :])
        up_copy[i].wait()
        up_act += mm(lhs[:, cols], up[cols, :])
    act = (gate_act / (1.0 + jnp.exp(-gate_act)) * up_act).astype(BF16)
    for i in range(chunks):
        down_copy[i].wait()
        result = mm(act, down[:, i * step : (i + 1) * step])
        for t in range(step // LANES):
            c = i * (step // LANES) + t
            for b in range(4):
                wide.at[b][pl.ds(c, rows, stride=tiles), :] = result[
                    b * rows : (b + 1) * rows, t * LANES : (t + 1) * LANES
                ]
    for b in range(4):
        out_refs[b][...] = wide[b].astype(BF16)


def combine_body(
    experts, back_ref, normed_ref, ids_ref, weights_ref, gain_ref, bias_ref, out_ref, wide_ref, rows_ref
):
    tokens, width = normed_ref.shape
    tiles = width // LANES
    top = ids_ref.shape[1]
    capacity = top * tokens // experts
    wide_ref[...] = back_ref[...].astype(F32)
    expert = lax.broadcasted_iota(jnp.int32, (tokens, experts), 1)
    named = jnp.zeros((tokens, experts), F32)
    weighted = jnp.zeros((tokens, experts), F32)
    for k in range(top):
        hit = ids_ref[:, k : k + 1] == expert
        named += hit.astype(F32)
        weighted += jnp.where(hit, weights_ref[:, k : k + 1], 0.0)
    earlier = lax.broadcasted_iota(jnp.int32, (tokens, tokens), 1) < lax.broadcasted_iota(
        jnp.int32, (tokens, tokens), 0
    )
    rank = mm(earlier.astype(BF16), named.astype(BF16))
    moe_sum = 0.0
    for j in range(capacity):
        pick = jnp.where((named > 0.5) & (jnp.abs(rank - j) < 0.5), weighted, 0.0)
        for c in range(tiles):
            rows_ref[:, c * LANES : (c + 1) * LANES] = wide_ref[
                pl.ds(j * tiles + c, experts, stride=capacity * tiles), :
            ].astype(BF16)
        high = pick.astype(BF16)
        low = pick - high.astype(F32)
        middle = low.astype(BF16)
        last = (low - middle.astype(F32)).astype(BF16)
        rows = rows_ref[...]
        moe_sum = moe_sum + (mm(high, rows) + (mm(middle, rows) + mm(last, rows)))
    pre_final = RESIDUAL_SCALE * normed_ref[...].astype(F32) + moe_sum
    out_ref[...] = layer_norm(pre_final, gain_ref[...], bias_ref[...]).astype(BF16)


def per_device(
    resid,
    queries,
    keys,
    values,
    doc_ids,
    sink_logits,
    out_proj,
    norm1_gain,
    norm1_bias,
    route_ids,
    route_weights,
    expert_gate,
    expert_up,
    expert_down,
    norm2_gain,
    norm2_bias,
):
    tokens = queries.shape[0]
    own, width = resid.shape
    blocks, members = lax.axis_size("sp"), lax.axis_size("tp")
    experts = blocks
    capacity = route_ids.shape[1] * own // experts
    tiles = width // LANES
    packed = experts * capacity * tiles

    keys_t, values_t, docs = keys.T, values.T, doc_ids.reshape(1, tokens)
    pack = shape((2 * HEAD_DIM + 16, WINDOW), BF16)
    head, tail = call(pack_body, [pack, pack], keys_t, values_t, docs, name="pack", flops=10**5)
    previous = lax.ppermute(tail, "sp", [(i, i + 1) for i in range(blocks - 1)])
    following = lax.ppermute(head, "sp", [(i + 1, i) for i in range(blocks - 1)])
    (partial,) = call(
        attention_body,
        [shape((tokens, width), BF16)],
        sink_logits.reshape(1, -1),
        queries,
        keys_t,
        values_t,
        docs,
        previous,
        following,
        out_proj,
        name="attend",
        flops=10**9,
        specs=[pl.BlockSpec(memory_space=pltpu.SMEM)] + [VMEM] * 7,
        scratch=[pltpu.VMEM(queries.shape, BF16)],
    )
    parts = lax.all_to_all(partial.reshape(members, own, width), "tp", 0, 0, tiled=True)
    normed, sent = call(
        functools.partial(dispatch_body, experts),
        [shape((own, width), BF16), shape((packed, LANES), BF16)],
        parts,
        resid,
        norm1_gain.reshape(1, -1),
        norm1_bias.reshape(1, -1),
        route_ids.T,
        name="dispatch",
        flops=10**9,
        scratch=[pltpu.VMEM((packed, LANES), F32)],
    )
    arrived = lax.all_to_all(sent, "sp", 0, 0, tiled=True)

    def turned(array, by):
        return lax.ppermute(array, "tp", [(i, (i + by) % members) for i in range(members)])

    hidden = expert_gate.shape[2]
    gathered = [arrived] + [turned(arrived, by) for by in range(1, members)]
    chunks = 4
    partials = call(
        expert_body,
        [shape((packed, LANES), BF16)] * members,
        *gathered,
        expert_gate[0],
        expert_up[0],
        expert_down[0],
        name="experts",
        flops=4 * 10**9,
        specs=[VMEM] * members + [ANY] * 3,
        scratch=[
            pltpu.VMEM((width, hidden), BF16),
            pltpu.VMEM((width, hidden), BF16),
            pltpu.VMEM((hidden, width), BF16),
            pltpu.VMEM((members * experts * capacity, width), BF16),
            pltpu.VMEM((members, packed, LANES), F32),
            pltpu.SemaphoreType.DMA((chunks,)),
            pltpu.SemaphoreType.DMA((chunks,)),
            pltpu.SemaphoreType.DMA((chunks,)),
        ],
    )
    summed = partials[0].astype(F32)
    for by in range(1, members):
        summed = summed + turned(partials[by], -by).astype(F32)
    back = lax.all_to_all(summed.astype(BF16), "sp", 0, 0, tiled=True)
    (mixed,) = call(
        functools.partial(combine_body, experts),
        [shape((own, width), BF16)],
        back,
        normed,
        route_ids,
        route_weights,
        norm2_gain.reshape(1, -1),
        norm2_bias.reshape(1, -1),
        name="combine",
        flops=10**9,
        scratch=[pltpu.VMEM((packed, LANES), F32), pltpu.VMEM((experts, width), BF16)],
    )
    return mixed


def solution(mesh):
    every = ("grp", "sp", "tp")
    group = ("grp", "sp")
    placed = (
        P(every, None),
        P(group, "tp"),
        P(group, "tp"),
        P(group, "tp"),
        P(group),
        P("tp"),
        P("tp", None),
        P(),
        P(),
        P(every, None),
        P(every, None),
        P("sp", None, "tp"),
        P("sp", None, "tp"),
        P("sp", "tp", None),
        P(),
        P(),
    )
    return jax.shard_map(
        per_device, mesh=mesh, in_specs=placed, out_specs=P(every, None), check_vma=False
    )
```

```python
import functools

import jax
import jax.numpy as jnp
from jax import lax
from jax.experimental import pallas as pl
from jax.experimental.pallas import tpu as pltpu
from jax.sharding import PartitionSpec as P

HEAD_DIM = 64
WINDOW = 128
LANES = 128
NORM_EPSILON = 1e-05
RESIDUAL_SCALE = 1.4142135623730951
MASKED = -1e30
F32 = jnp.float32
BF16 = jnp.bfloat16


VMEM = pl.BlockSpec(memory_space=pltpu.VMEM)


def mm(a, b):
    return jnp.dot(a, b, preferred_element_type=F32)


def mm_nt(a, b):
    return lax.dot_general(a, b, (((1,), (1,)), ((), ())), preferred_element_type=F32)


def call(body, out_shapes, *args, name, flops, specs=None, scratch=(), vmem=None):
    size = sum(a.size * a.dtype.itemsize for a in args)
    size += sum(s.size * s.dtype.itemsize for s in out_shapes)
    return pl.pallas_call(
        body,
        out_shape=out_shapes,
        in_specs=specs or [VMEM] * len(args),
        out_specs=[VMEM] * len(out_shapes),
        scratch_shapes=list(scratch),
        compiler_params=pltpu.CompilerParams(vmem_limit_bytes=vmem or 12 * 2**20),
        cost_estimate=pl.CostEstimate(flops=flops, bytes_accessed=size, transcendentals=0),
        name=name,
    )(*args)


def shape(dims, dtype):
    return jax.ShapeDtypeStruct(dims, dtype)


def layer_norm(values, gain, bias):
    centred = values - jnp.mean(values, -1, keepdims=True)
    variance = jnp.mean(centred * centred, -1, keepdims=True)
    return centred * lax.rsqrt(variance + NORM_EPSILON) * gain + bias


def pack_body(keys_ref, values_ref, docs_ref, head_ref, tail_ref):
    tokens = keys_ref.shape[1]
    docs = (docs_ref[...].astype(F32) + 1.0).astype(BF16)
    for ref, lo in ((head_ref, 0), (tail_ref, tokens - WINDOW)):
        cols = slice(lo, lo + WINDOW)
        ref[0:HEAD_DIM, :] = keys_ref[:, cols]
        ref[HEAD_DIM : 2 * HEAD_DIM, :] = values_ref[:, cols]
        ref[2 * HEAD_DIM :, :] = jnp.broadcast_to(docs[:, cols], (16, WINDOW))


def attention_body(
    sink_ref, query_ref, keys_ref, values_ref, docs_ref, prev_ref, next_ref, proj_ref, out_ref, att_ref
):
    tokens = query_ref.shape[0]
    heads = query_ref.shape[1] // HEAD_DIM
    own_docs = docs_ref[...].astype(F32) + 1.0
    query_docs = jnp.broadcast_to(own_docs, (LANES, tokens)).T[:, 0:1]
    row = lax.broadcasted_iota(jnp.int32, (tokens, 1), 0)
    blocks = []
    for key, value, docs, first in (
        (prev_ref[0:HEAD_DIM, :], prev_ref[HEAD_DIM : 2 * HEAD_DIM, :], None, -WINDOW),
        (keys_ref[...], values_ref[...], own_docs, 0),
        (next_ref[0:HEAD_DIM, :], next_ref[HEAD_DIM : 2 * HEAD_DIM, :], None, tokens),
    ):
        if docs is None:
            ref = prev_ref if first < 0 else next_ref
            docs = ref[2 * HEAD_DIM :, :].astype(F32)[0:1, :]
        width = key.shape[1]
        place = first + lax.broadcasted_iota(jnp.int32, (1, width), 1)
        allowed = (jnp.abs(row - place) <= WINDOW) & (query_docs == docs)
        blocks.append((key, value, allowed))
    for h in range(heads):
        cols = slice(h * HEAD_DIM, (h + 1) * HEAD_DIM)
        query = query_ref[:, cols]
        sink = sink_ref[0, h]
        scores = [
            jnp.where(allowed, mm(query, key) * HEAD_DIM ** (-0.5), MASKED)
            for key, _, allowed in blocks
        ]
        top = functools.reduce(jnp.maximum, [jnp.max(s, -1, keepdims=True) for s in scores])
        top = jnp.maximum(top, sink)
        raised = [
            jnp.where(allowed, jnp.exp(s - top), 0.0) for s, (_, _, allowed) in zip(scores, blocks)
        ]
        total = jnp.exp(sink - top) + sum(jnp.sum(r, -1, keepdims=True) for r in raised)
        scale = 1.0 / total
        result = sum(
            mm_nt((r * scale).astype(BF16), value) for r, (_, value, _) in zip(raised, blocks)
        )
        att_ref[:, cols] = result.astype(BF16)
    out_ref[...] = mm(att_ref[...], proj_ref[...]).astype(BF16)


def routing_rows(ids, experts, tokens):
    expert = lax.broadcasted_iota(jnp.int32, (experts, tokens), 0)
    named = jnp.zeros((experts, tokens), F32)
    for k in range(ids.shape[0]):
        named += (ids[k : k + 1, :] == expert).astype(F32)
    before = lax.broadcasted_iota(jnp.int32, (tokens, tokens), 0) < lax.broadcasted_iota(
        jnp.int32, (tokens, tokens), 1
    )
    rank = mm(named.astype(BF16), before.astype(BF16))
    return named, rank


def dispatch_body(
    experts, parts_ref, resid_ref, gain_ref, bias_ref, ids_ref, normed_ref, sent_ref, wide_ref
):
    tokens, width = resid_ref.shape
    tiles = width // LANES
    capacity = ids_ref.shape[0] * tokens // experts
    projected = sum(parts_ref[i].astype(F32) for i in range(parts_ref.shape[0]))
    pre_norm = RESIDUAL_SCALE * resid_ref[...].astype(F32) + projected.astype(BF16).astype(F32)
    normed = layer_norm(pre_norm, gain_ref[...], bias_ref[...]).astype(BF16)
    normed_ref[...] = normed
    named, rank = routing_rows(ids_ref[...], experts, tokens)
    for j in range(capacity):
        pick = jnp.where((named > 0.5) & (jnp.abs(rank - j) < 0.5), 1.0, 0.0).astype(BF16)
        rows = mm(pick, normed)
        for c in range(tiles):
            wide_ref[pl.ds(j * tiles + c, experts, stride=capacity * tiles), :] = rows[
                :, c * LANES : (c + 1) * LANES
            ]
    sent_ref[...] = wide_ref[...].astype(BF16)


def expert_body(count, *refs):
    row_refs, (gate_ref, up_ref, down_ref), refs = refs[:count], refs[count : count + 3], refs[count + 3 :]
    out_refs, (lhs, wide) = refs[:count], refs[count:]
    tiles = gate_ref.shape[0] // LANES
    rows = row_refs[0].shape[0] // tiles
    for b, ref in enumerate(row_refs):
        wide[b] = ref[...].astype(F32)
        for c in range(tiles):
            lhs[b * rows : (b + 1) * rows, c * LANES : (c + 1) * LANES] = wide.at[b][
                pl.ds(c, rows, stride=tiles), :
            ].astype(BF16)
    gate_act = mm(lhs[...], gate_ref[...])
    up_act = mm(lhs[...], up_ref[...])
    act = (gate_act / (1.0 + jnp.exp(-gate_act)) * up_act).astype(BF16)
    step = 4 * LANES
    for i in range(0, down_ref.shape[1], step):
        result = mm(act, down_ref[:, i : i + step])
        for t in range(0, step, LANES):
            for b in range(count):
                wide.at[b][pl.ds((i + t) // LANES, rows, stride=tiles), :] = result[
                    b * rows : (b + 1) * rows, t : t + LANES
                ]
    for b in range(count):
        out_refs[b][...] = wide[b].astype(BF16)


def combine_body(
    experts, back_ref, normed_ref, ids_ref, weights_ref, gain_ref, bias_ref, out_ref, wide_ref, rows_ref
):
    tokens, width = normed_ref.shape
    tiles = width // LANES
    top = ids_ref.shape[1]
    capacity = top * tokens // experts
    wide_ref[...] = back_ref[...].astype(F32)
    expert = lax.broadcasted_iota(jnp.int32, (tokens, experts), 1)
    named = jnp.zeros((tokens, experts), F32)
    weighted = jnp.zeros((tokens, experts), F32)
    for k in range(top):
        hit = ids_ref[:, k : k + 1] == expert
        named += hit.astype(F32)
        weighted += jnp.where(hit, weights_ref[:, k : k + 1], 0.0)
    earlier = lax.broadcasted_iota(jnp.int32, (tokens, tokens), 1) < lax.broadcasted_iota(
        jnp.int32, (tokens, tokens), 0
    )
    rank = mm(earlier.astype(BF16), named.astype(BF16))
    moe_sum = 0.0
    for j in range(capacity):
        pick = jnp.where((named > 0.5) & (jnp.abs(rank - j) < 0.5), weighted, 0.0)
        for c in range(tiles):
            rows_ref[:, c * LANES : (c + 1) * LANES] = wide_ref[
                pl.ds(j * tiles + c, experts, stride=capacity * tiles), :
            ].astype(BF16)
        high = pick.astype(BF16)
        low = pick - high.astype(F32)
        middle = low.astype(BF16)
        last = (low - middle.astype(F32)).astype(BF16)
        rows = rows_ref[...]
        moe_sum = moe_sum + (mm(high, rows) + (mm(middle, rows) + mm(last, rows)))
    pre_final = RESIDUAL_SCALE * normed_ref[...].astype(F32) + moe_sum
    out_ref[...] = layer_norm(pre_final, gain_ref[...], bias_ref[...]).astype(BF16)


def per_device(
    resid,
    queries,
    keys,
    values,
    doc_ids,
    sink_logits,
    out_proj,
    norm1_gain,
    norm1_bias,
    route_ids,
    route_weights,
    expert_gate,
    expert_up,
    expert_down,
    norm2_gain,
    norm2_bias,
):
    tokens = queries.shape[0]
    own, width = resid.shape
    blocks, members = lax.axis_size("sp"), lax.axis_size("tp")
    experts = blocks
    capacity = route_ids.shape[1] * own // experts
    tiles = width // LANES
    packed = experts * capacity * tiles

    keys_t, values_t, docs = keys.T, values.T, doc_ids.reshape(1, tokens)
    pack = shape((2 * HEAD_DIM + 16, WINDOW), BF16)
    head, tail = call(pack_body, [pack, pack], keys_t, values_t, docs, name="pack", flops=10**5)
    previous = lax.ppermute(tail, "sp", [(i, i + 1) for i in range(blocks - 1)])
    following = lax.ppermute(head, "sp", [(i + 1, i) for i in range(blocks - 1)])
    (partial,) = call(
        attention_body,
        [shape((tokens, width), BF16)],
        sink_logits.reshape(1, -1),
        queries,
        keys_t,
        values_t,
        docs,
        previous,
        following,
        out_proj,
        name="attend",
        flops=10**9,
        specs=[pl.BlockSpec(memory_space=pltpu.SMEM)] + [VMEM] * 7,
        scratch=[pltpu.VMEM(queries.shape, BF16)],
    )
    parts = lax.all_to_all(partial.reshape(members, own, width), "tp", 0, 0, tiled=True)
    normed, sent = call(
        functools.partial(dispatch_body, experts),
        [shape((own, width), BF16), shape((packed, LANES), BF16)],
        parts,
        resid,
        norm1_gain.reshape(1, -1),
        norm1_bias.reshape(1, -1),
        route_ids.T,
        name="dispatch",
        flops=10**9,
        scratch=[pltpu.VMEM((packed, LANES), F32)],
    )
    arrived = lax.all_to_all(sent, "sp", 0, 0, tiled=True)

    def turned(array, by):
        return lax.ppermute(array, "tp", [(i, (i + by) % members) for i in range(members)])

    def expert(*row_sets):
        count = len(row_sets)
        return call(
            functools.partial(expert_body, count),
            [shape((packed, LANES), BF16)] * count,
            *row_sets,
            expert_gate[0],
            expert_up[0],
            expert_down[0],
            name="experts",
            flops=count * 10**9,
            scratch=[
                pltpu.VMEM((count * experts * capacity, width), BF16),
                pltpu.VMEM((count, packed, LANES), F32),
            ],
        )

    steps = [by for by in range(1, members)]
    moved = {by: turned(arrived, by) for by in steps}
    near = [1, members - 1]
    far = [by for by in steps if by not in near]
    (kept,) = expert(arrived)
    results = dict(zip(near, expert(*[moved[by] for by in near])))
    results.update(zip(far, expert(*[moved[by] for by in far])))
    summed = kept.astype(F32)
    for by in steps:
        summed = summed + turned(results[by], -by).astype(F32)
    back = lax.all_to_all(summed.astype(BF16), "sp", 0, 0, tiled=True)
    (mixed,) = call(
        functools.partial(combine_body, experts),
        [shape((own, width), BF16)],
        back,
        normed,
        route_ids,
        route_weights,
        norm2_gain.reshape(1, -1),
        norm2_bias.reshape(1, -1),
        name="combine",
        flops=10**9,
        scratch=[pltpu.VMEM((packed, LANES), F32), pltpu.VMEM((experts, width), BF16)],
    )
    return mixed


def solution(mesh):
    every = ("grp", "sp", "tp")
    group = ("grp", "sp")
    placed = (
        P(every, None),
        P(group, "tp"),
        P(group, "tp"),
        P(group, "tp"),
        P(group),
        P("tp"),
        P("tp", None),
        P(),
        P(),
        P(every, None),
        P(every, None),
        P("sp", None, "tp"),
        P("sp", None, "tp"),
        P("sp", "tp", None),
        P(),
        P(),
    )
    return jax.shard_map(
        per_device, mesh=mesh, in_specs=placed, out_specs=P(every, None), check_vma=False
    )
```

```python
import functools

import jax
import jax.numpy as jnp
from jax import lax
from jax.experimental import pallas as pl
from jax.experimental.pallas import tpu as pltpu
from jax.sharding import PartitionSpec as P

HEAD_DIM = 64
WINDOW = 128
LANES = 128
NORM_EPSILON = 1e-05
RESIDUAL_SCALE = 1.4142135623730951
MASKED = -1e30
F32 = jnp.float32
BF16 = jnp.bfloat16


VMEM = pl.BlockSpec(memory_space=pltpu.VMEM)
HBM = pl.BlockSpec(memory_space=pltpu.HBM)


def mm(a, b):
    return jnp.dot(a, b, preferred_element_type=F32)


def mm_nt(a, b):
    return lax.dot_general(a, b, (((1,), (1,)), ((), ())), preferred_element_type=F32)


def call(body, out_shapes, *args, name, flops, specs=None, scratch=(), vmem=None):
    size = sum(a.size * a.dtype.itemsize for a in args)
    size += sum(s.size * s.dtype.itemsize for s in out_shapes)
    return pl.pallas_call(
        body,
        out_shape=out_shapes,
        in_specs=specs or [VMEM] * len(args),
        out_specs=[VMEM] * len(out_shapes),
        scratch_shapes=list(scratch),
        compiler_params=pltpu.CompilerParams(vmem_limit_bytes=vmem or 12 * 2**20),
        cost_estimate=pl.CostEstimate(flops=flops, bytes_accessed=size, transcendentals=0),
        name=name,
    )(*args)


def shape(dims, dtype):
    return jax.ShapeDtypeStruct(dims, dtype)


def layer_norm(values, gain, bias):
    centred = values - jnp.mean(values, -1, keepdims=True)
    variance = jnp.mean(centred * centred, -1, keepdims=True)
    return centred * lax.rsqrt(variance + NORM_EPSILON) * gain + bias


def first_body(count, *refs):
    sources, held, (head_ref, tail_ref, sems) = refs[:count], refs[count : 2 * count], refs[2 * count :]
    copies = [pltpu.make_async_copy(a, b, sems.at[i]) for i, (a, b) in enumerate(zip(sources, held))]
    for copy in copies:
        copy.start()
    for copy in copies[:3]:
        copy.wait()
    keys_ref, values_ref, docs_ref = held[:3]
    tokens = keys_ref.shape[1]
    docs = (docs_ref[...].astype(F32) + 1.0).astype(BF16)
    for ref, lo in ((head_ref, 0), (tail_ref, tokens - WINDOW)):
        cols = slice(lo, lo + WINDOW)
        ref[0:HEAD_DIM, :] = keys_ref[:, cols]
        ref[HEAD_DIM : 2 * HEAD_DIM, :] = values_ref[:, cols]
        ref[2 * HEAD_DIM :, :] = jnp.broadcast_to(docs[:, cols], (16, WINDOW))
    for copy in copies[3:]:
        copy.wait()


def attention_body(
    sink_ref, query_ref, keys_ref, values_ref, docs_ref, prev_ref, next_ref, proj_ref, out_ref, att_ref
):
    tokens = query_ref.shape[0]
    heads = query_ref.shape[1] // HEAD_DIM
    own_docs = docs_ref[...].astype(F32) + 1.0
    query_docs = jnp.broadcast_to(own_docs, (LANES, tokens)).T[:, 0:1]
    row = lax.broadcasted_iota(jnp.int32, (tokens, 1), 0)
    blocks = []
    for key, value, docs, first in (
        (prev_ref[0:HEAD_DIM, :], prev_ref[HEAD_DIM : 2 * HEAD_DIM, :], None, -WINDOW),
        (keys_ref[...], values_ref[...], own_docs, 0),
        (next_ref[0:HEAD_DIM, :], next_ref[HEAD_DIM : 2 * HEAD_DIM, :], None, tokens),
    ):
        if docs is None:
            ref = prev_ref if first < 0 else next_ref
            docs = ref[2 * HEAD_DIM :, :].astype(F32)[0:1, :]
        width = key.shape[1]
        place = first + lax.broadcasted_iota(jnp.int32, (1, width), 1)
        allowed = (jnp.abs(row - place) <= WINDOW) & (query_docs == docs)
        blocks.append((key, value, allowed))
    for h in range(heads):
        cols = slice(h * HEAD_DIM, (h + 1) * HEAD_DIM)
        query = query_ref[:, cols]
        sink = sink_ref[:, h : h + 1]
        scores = [
            jnp.where(allowed, mm(query, key) * HEAD_DIM ** (-0.5), MASKED)
            for key, _, allowed in blocks
        ]
        top = functools.reduce(jnp.maximum, [jnp.max(s, -1, keepdims=True) for s in scores])
        top = jnp.maximum(top, sink)
        raised = [
            jnp.where(allowed, jnp.exp(s - top), 0.0) for s, (_, _, allowed) in zip(scores, blocks)
        ]
        total = jnp.exp(sink - top) + sum(jnp.sum(r, -1, keepdims=True) for r in raised)
        scale = 1.0 / total
        result = sum(
            mm_nt((r * scale).astype(BF16), value) for r, (_, value, _) in zip(raised, blocks)
        )
        att_ref[:, cols] = result.astype(BF16)
    out_ref[...] = mm(att_ref[...], proj_ref[...]).astype(BF16)


def routing_rows(ids, experts, tokens):
    expert = lax.broadcasted_iota(jnp.int32, (experts, tokens), 0)
    named = jnp.zeros((experts, tokens), F32)
    for k in range(ids.shape[0]):
        named += (ids[k : k + 1, :] == expert).astype(F32)
    before = lax.broadcasted_iota(jnp.int32, (tokens, tokens), 0) < lax.broadcasted_iota(
        jnp.int32, (tokens, tokens), 1
    )
    rank = mm(named.astype(BF16), before.astype(BF16))
    return named, rank


def dispatch_body(
    experts, parts_ref, resid_ref, gain_ref, bias_ref, ids_ref, normed_ref, sent_ref, wide_ref
):
    tokens, width = resid_ref.shape
    tiles = width // LANES
    capacity = ids_ref.shape[0] * tokens // experts
    projected = sum(parts_ref[i].astype(F32) for i in range(parts_ref.shape[0]))
    pre_norm = RESIDUAL_SCALE * resid_ref[...].astype(F32) + projected.astype(BF16).astype(F32)
    normed = layer_norm(pre_norm, gain_ref[...], bias_ref[...]).astype(BF16)
    normed_ref[...] = normed
    named, rank = routing_rows(ids_ref[...], experts, tokens)
    for j in range(capacity):
        pick = jnp.where((named > 0.5) & (jnp.abs(rank - j) < 0.5), 1.0, 0.0).astype(BF16)
        rows = mm(pick, normed)
        for c in range(tiles):
            wide_ref[pl.ds(j * tiles + c, experts, stride=capacity * tiles), :] = rows[
                :, c * LANES : (c + 1) * LANES
            ]
    sent_ref[...] = wide_ref[...].astype(BF16)


def expert_body(count, *refs):
    row_refs, (gate_ref, up_ref, down_ref), refs = refs[:count], refs[count : count + 3], refs[count + 3 :]
    out_refs, (lhs, wide) = refs[:count], refs[count:]
    tiles = gate_ref.shape[0] // LANES
    rows = row_refs[0].shape[0] // tiles
    for b, ref in enumerate(row_refs):
        wide[b] = ref[...].astype(F32)
        for c in range(tiles):
            lhs[b * rows : (b + 1) * rows, c * LANES : (c + 1) * LANES] = wide.at[b][
                pl.ds(c, rows, stride=tiles), :
            ].astype(BF16)
    gate_act = mm(lhs[...], gate_ref[...])
    up_act = mm(lhs[...], up_ref[...])
    act = (gate_act / (1.0 + jnp.exp(-gate_act)) * up_act).astype(BF16)
    step = 4 * LANES
    for i in range(0, down_ref.shape[1], step):
        result = mm(act, down_ref[:, i : i + step])
        for t in range(0, step, LANES):
            for b in range(count):
                wide.at[b][pl.ds((i + t) // LANES, rows, stride=tiles), :] = result[
                    b * rows : (b + 1) * rows, t : t + LANES
                ]
    for b in range(count):
        out_refs[b][...] = wide[b].astype(BF16)


def total_body(kept_ref, left_1_ref, right_1_ref, left_2_ref, right_2_ref, out_ref):
    half = left_1_ref.shape[0]
    for part, left_ref, right_ref in ((0, left_1_ref, right_1_ref), (1, left_2_ref, right_2_ref)):
        rows = slice(part * half, (part + 1) * half)
        sides = left_ref[...].astype(F32) + right_ref[...].astype(F32)
        out_ref[rows, :] = (kept_ref[rows, :].astype(F32) + sides).astype(BF16)


def combine_body(
    experts, back_ref, normed_ref, ids_ref, weights_ref, gain_ref, bias_ref, out_ref, wide_ref, rows_ref
):
    tokens, width = normed_ref.shape
    tiles = width // LANES
    top = ids_ref.shape[1]
    capacity = top * tokens // experts
    wide_ref[...] = back_ref[...].astype(F32)
    expert = lax.broadcasted_iota(jnp.int32, (tokens, experts), 1)
    named = jnp.zeros((tokens, experts), F32)
    weighted = jnp.zeros((tokens, experts), F32)
    for k in range(top):
        hit = ids_ref[:, k : k + 1] == expert
        named += hit.astype(F32)
        weighted += jnp.where(hit, weights_ref[:, k : k + 1], 0.0)
    earlier = lax.broadcasted_iota(jnp.int32, (tokens, tokens), 1) < lax.broadcasted_iota(
        jnp.int32, (tokens, tokens), 0
    )
    rank = mm(earlier.astype(BF16), named.astype(BF16))
    moe_sum = 0.0
    for j in range(capacity):
        pick = jnp.where((named > 0.5) & (jnp.abs(rank - j) < 0.5), weighted, 0.0)
        for c in range(tiles):
            rows_ref[:, c * LANES : (c + 1) * LANES] = wide_ref[
                pl.ds(j * tiles + c, experts, stride=capacity * tiles), :
            ].astype(BF16)
        high = pick.astype(BF16)
        low = pick - high.astype(F32)
        middle = low.astype(BF16)
        last = (low - middle.astype(F32)).astype(BF16)
        rows = rows_ref[...]
        moe_sum = moe_sum + (mm(high, rows) + (mm(middle, rows) + mm(last, rows)))
    pre_final = RESIDUAL_SCALE * normed_ref[...].astype(F32) + moe_sum
    out_ref[...] = layer_norm(pre_final, gain_ref[...], bias_ref[...]).astype(BF16)


def per_device(
    resid,
    queries,
    keys,
    values,
    doc_ids,
    sink_logits,
    out_proj,
    norm1_gain,
    norm1_bias,
    route_ids,
    route_weights,
    expert_gate,
    expert_up,
    expert_down,
    norm2_gain,
    norm2_bias,
):
    tokens = queries.shape[0]
    own, width = resid.shape
    blocks, members = lax.axis_size("sp"), lax.axis_size("tp")
    experts = blocks
    capacity = route_ids.shape[1] * own // experts
    tiles = width // LANES
    packed = experts * capacity * tiles

    small = (keys.T, values.T, doc_ids.reshape(1, tokens), queries, out_proj, resid, sink_logits.reshape(1, -1))
    pack = shape((2 * HEAD_DIM + 16, WINDOW), BF16)
    keys_t, values_t, docs, queries, out_proj, resid, sinks, head, tail = call(
        functools.partial(first_body, len(small)),
        [shape(a.shape, a.dtype) for a in small] + [pack, pack],
        *[pltpu.with_memory_space_constraint(a, pltpu.HBM) for a in small],
        name="first",
        flops=10**5,
        specs=[HBM] * len(small),
        scratch=[pltpu.SemaphoreType.DMA((len(small),))],
    )
    previous = lax.ppermute(tail, "sp", [(i, i + 1) for i in range(blocks - 1)])
    following = lax.ppermute(head, "sp", [(i + 1, i) for i in range(blocks - 1)])
    (partial,) = call(
        attention_body,
        [shape((tokens, width), BF16)],
        sinks,
        queries,
        keys_t,
        values_t,
        docs,
        previous,
        following,
        out_proj,
        name="attend",
        flops=10**9,
        scratch=[pltpu.VMEM(queries.shape, BF16)],
    )
    parts = lax.all_to_all(partial.reshape(members, own, width), "tp", 0, 0, tiled=True)
    normed, sent = call(
        functools.partial(dispatch_body, experts),
        [shape((own, width), BF16), shape((packed, LANES), BF16)],
        parts,
        resid,
        norm1_gain.reshape(1, -1),
        norm1_bias.reshape(1, -1),
        route_ids.T,
        name="dispatch",
        flops=10**9,
        scratch=[pltpu.VMEM((packed, LANES), F32)],
    )
    arrived = lax.all_to_all(sent, "sp", 0, 0, tiled=True)

    def turned(array, by):
        return lax.ppermute(array, "tp", [(i, (i + by) % members) for i in range(members)])

    def expert(*row_sets):
        count, rows = len(row_sets), row_sets[0].shape[0]
        return call(
            functools.partial(expert_body, count),
            [shape((rows, LANES), BF16)] * count,
            *row_sets,
            expert_gate[0],
            expert_up[0],
            expert_down[0],
            name="experts",
            flops=count * rows * 10**6,
            scratch=[
                pltpu.VMEM((count * rows // tiles, width), BF16),
                pltpu.VMEM((count, rows, LANES), F32),
            ],
        )

    half = packed // 2
    first, second = arrived[:half], arrived[half:]
    left_1, right_2 = turned(first, 1), turned(second, -1)
    left_2, right_1 = turned(second, 1), turned(first, -1)
    far_1, far_2 = turned(left_1, 1), turned(right_2, -1)
    (kept,) = expert(arrived)
    for_left_1, for_left_2, for_right_1, for_right_2 = expert(left_1, left_2, right_1, right_2)
    for_far_1, for_far_2 = expert(far_1, far_2)
    from_right_2, from_left_1 = turned(for_left_2, -1), turned(for_right_1, 1)
    for_left_1 = for_left_1.astype(F32) + turned(for_far_1, -1).astype(F32)
    for_right_2 = for_right_2.astype(F32) + turned(for_far_2, 1).astype(F32)
    from_right_1 = turned(for_left_1.astype(BF16), -1)
    from_left_2 = turned(for_right_2.astype(BF16), 1)
    (summed,) = call(
        total_body,
        [shape((packed, LANES), BF16)],
        kept,
        from_left_1,
        from_right_1,
        from_left_2,
        from_right_2,
        name="total",
        flops=10**7,
    )
    back = lax.all_to_all(summed, "sp", 0, 0, tiled=True)
    (mixed,) = call(
        functools.partial(combine_body, experts),
        [shape((own, width), BF16)],
        back,
        normed,
        route_ids,
        route_weights,
        norm2_gain.reshape(1, -1),
        norm2_bias.reshape(1, -1),
        name="combine",
        flops=10**9,
        scratch=[pltpu.VMEM((packed, LANES), F32), pltpu.VMEM((experts, width), BF16)],
    )
    return mixed


def solution(mesh):
    every = ("grp", "sp", "tp")
    group = ("grp", "sp")
    placed = (
        P(every, None),
        P(group, "tp"),
        P(group, "tp"),
        P(group, "tp"),
        P(group),
        P("tp"),
        P("tp", None),
        P(),
        P(),
        P(every, None),
        P(every, None),
        P("sp", None, "tp"),
        P("sp", None, "tp"),
        P("sp", "tp", None),
        P(),
        P(),
    )
    return jax.shard_map(
        per_device, mesh=mesh, in_specs=placed, out_specs=P(every, None), check_vma=False
    )
```

```python
import functools

import jax
import jax.numpy as jnp
from jax import lax
from jax.experimental import pallas as pl
from jax.experimental.pallas import tpu as pltpu
from jax.sharding import PartitionSpec as P


HEAD_DIM = 64
WINDOW = 128
LANES = 128
NORM_EPSILON = 1e-05
RESIDUAL_SCALE = 1.4142135623730951
MASKED = -1e30
F32 = jnp.float32
BF16 = jnp.bfloat16


VMEM = pl.BlockSpec(memory_space=pltpu.VMEM)
HBM = pl.BlockSpec(memory_space=pltpu.HBM)


def mm(a, b):
    return jnp.dot(a, b, preferred_element_type=F32)


def mm_nt(a, b):
    return lax.dot_general(a, b, (((1,), (1,)), ((), ())), preferred_element_type=F32)


def call(body, out_shapes, *args, flops, specs=None, scratch=(), vmem=None):
    size = sum(a.size * a.dtype.itemsize for a in args)
    size += sum(s.size * s.dtype.itemsize for s in out_shapes)
    return pl.pallas_call(
        body,
        out_shape=out_shapes,
        in_specs=specs or [VMEM] * len(args),
        out_specs=[VMEM] * len(out_shapes),
        scratch_shapes=list(scratch),
        compiler_params=pltpu.CompilerParams(vmem_limit_bytes=vmem or 12 * 2**20),
        cost_estimate=pl.CostEstimate(flops=flops, bytes_accessed=size, transcendentals=0),
    )(*args)


def shape(dims, dtype):
    return jax.ShapeDtypeStruct(dims, dtype)


def layer_norm(values, gain, bias):
    centred = values - jnp.mean(values, -1, keepdims=True)
    variance = jnp.mean(centred * centred, -1, keepdims=True)
    return centred * lax.rsqrt(variance + NORM_EPSILON) * gain + bias


def first_body(count, *refs):
    sources, held, (head_ref, tail_ref, sems) = refs[:count], refs[count : 2 * count], refs[2 * count :]
    copies = [pltpu.make_async_copy(a, b, sems.at[i]) for i, (a, b) in enumerate(zip(sources, held))]
    for copy in copies:
        copy.start()
    for copy in copies[:3]:
        copy.wait()
    keys_ref, values_ref, docs_ref = held[:3]
    tokens = keys_ref.shape[1]
    docs = (docs_ref[...].astype(F32) + 1.0).astype(BF16)
    for ref, lo in ((head_ref, 0), (tail_ref, tokens - WINDOW)):
        cols = slice(lo, lo + WINDOW)
        ref[0:HEAD_DIM, :] = keys_ref[:, cols]
        ref[HEAD_DIM : 2 * HEAD_DIM, :] = values_ref[:, cols]
        ref[2 * HEAD_DIM :, :] = jnp.broadcast_to(docs[:, cols], (16, WINDOW))
    for copy in copies[3:]:
        copy.wait()


def attention_body(
    sink_ref, query_ref, keys_ref, values_ref, docs_ref, prev_ref, next_ref, proj_ref, out_ref, att_ref
):
    tokens = query_ref.shape[0]
    heads = query_ref.shape[1] // HEAD_DIM
    own_docs = docs_ref[...].astype(F32) + 1.0
    query_docs = jnp.broadcast_to(own_docs, (LANES, tokens)).T[:, 0:1]
    row = lax.broadcasted_iota(jnp.int32, (tokens, 1), 0)
    blocks = []
    for key, value, docs, first in (
        (prev_ref[0:HEAD_DIM, :], prev_ref[HEAD_DIM : 2 * HEAD_DIM, :], None, -WINDOW),
        (keys_ref[...], values_ref[...], own_docs, 0),
        (next_ref[0:HEAD_DIM, :], next_ref[HEAD_DIM : 2 * HEAD_DIM, :], None, tokens),
    ):
        if docs is None:
            ref = prev_ref if first < 0 else next_ref
            docs = ref[2 * HEAD_DIM :, :].astype(F32)[0:1, :]
        width = key.shape[1]
        place = first + lax.broadcasted_iota(jnp.int32, (1, width), 1)
        allowed = (jnp.abs(row - place) <= WINDOW) & (query_docs == docs)
        blocks.append((key, value, allowed))
    for h in range(heads):
        cols = slice(h * HEAD_DIM, (h + 1) * HEAD_DIM)
        query = query_ref[:, cols]
        sink = sink_ref[:, h : h + 1]
        scores = [
            jnp.where(allowed, mm(query, key) * HEAD_DIM ** (-0.5), MASKED)
            for key, _, allowed in blocks
        ]
        top = functools.reduce(jnp.maximum, [jnp.max(s, -1, keepdims=True) for s in scores])
        top = jnp.maximum(top, sink)
        raised = [
            jnp.where(allowed, jnp.exp(s - top), 0.0) for s, (_, _, allowed) in zip(scores, blocks)
        ]
        total = jnp.exp(sink - top) + sum(jnp.sum(r, -1, keepdims=True) for r in raised)
        scale = 1.0 / total
        result = sum(
            mm_nt((r * scale).astype(BF16), value) for r, (_, value, _) in zip(raised, blocks)
        )
        att_ref[:, cols] = result.astype(BF16)
    out_ref[...] = mm(att_ref[...], proj_ref[...]).astype(BF16)


def routing_rows(ids, experts, tokens):
    expert = lax.broadcasted_iota(jnp.int32, (experts, tokens), 0)
    named = jnp.zeros((experts, tokens), F32)
    for k in range(ids.shape[0]):
        named += (ids[k : k + 1, :] == expert).astype(F32)
    before = lax.broadcasted_iota(jnp.int32, (tokens, tokens), 0) < lax.broadcasted_iota(
        jnp.int32, (tokens, tokens), 1
    )
    rank = mm(named.astype(BF16), before.astype(BF16))
    return named, rank


def dispatch_body(
    experts, parts_ref, resid_ref, gain_ref, bias_ref, ids_ref, normed_ref, sent_ref, wide_ref
):
    tokens, width = resid_ref.shape
    tiles = width // LANES
    capacity = ids_ref.shape[0] * tokens // experts
    projected = sum(parts_ref[i].astype(F32) for i in range(parts_ref.shape[0]))
    pre_norm = RESIDUAL_SCALE * resid_ref[...].astype(F32) + projected.astype(BF16).astype(F32)
    normed = layer_norm(pre_norm, gain_ref[...], bias_ref[...]).astype(BF16)
    normed_ref[...] = normed
    named, rank = routing_rows(ids_ref[...], experts, tokens)
    for j in range(capacity):
        pick = jnp.where((named > 0.5) & (jnp.abs(rank - j) < 0.5), 1.0, 0.0).astype(BF16)
        rows = mm(pick, normed)
        for c in range(tiles):
            wide_ref[pl.ds(j * tiles + c, experts, stride=capacity * tiles), :] = rows[
                :, c * LANES : (c + 1) * LANES
            ]
    sent_ref[...] = wide_ref[...].astype(BF16)


def expert_body(count, *refs):
    row_refs, (gate_ref, up_ref, down_ref), refs = refs[:count], refs[count : count + 3], refs[count + 3 :]
    out_refs, (lhs, wide) = refs[:count], refs[count:]
    tiles = gate_ref.shape[0] // LANES
    rows = row_refs[0].shape[0] // tiles
    for b, ref in enumerate(row_refs):
        wide[b] = ref[...].astype(F32)
        for c in range(tiles):
            lhs[b * rows : (b + 1) * rows, c * LANES : (c + 1) * LANES] = wide.at[b][
                pl.ds(c, rows, stride=tiles), :
            ].astype(BF16)
    gate_act = mm(lhs[...], gate_ref[...])
    up_act = mm(lhs[...], up_ref[...])
    act = (gate_act / (1.0 + jnp.exp(-gate_act)) * up_act).astype(BF16)
    step = 4 * LANES
    for i in range(0, down_ref.shape[1], step):
        result = mm(act, down_ref[:, i : i + step])
        for t in range(0, step, LANES):
            for b in range(count):
                wide.at[b][pl.ds((i + t) // LANES, rows, stride=tiles), :] = result[
                    b * rows : (b + 1) * rows, t : t + LANES
                ]
    for b in range(count):
        out_refs[b][...] = wide[b].astype(BF16)


def total_body(kept_ref, left_1_ref, right_1_ref, left_2_ref, right_2_ref, out_ref):
    half = left_1_ref.shape[0]
    for part, left_ref, right_ref in ((0, left_1_ref, right_1_ref), (1, left_2_ref, right_2_ref)):
        rows = slice(part * half, (part + 1) * half)
        sides = left_ref[...].astype(F32) + right_ref[...].astype(F32)
        out_ref[rows, :] = (kept_ref[rows, :].astype(F32) + sides).astype(BF16)


def combine_body(
    experts, back_ref, normed_ref, ids_ref, weights_ref, gain_ref, bias_ref, out_ref, wide_ref, rows_ref
):
    tokens, width = normed_ref.shape
    tiles = width // LANES
    top = ids_ref.shape[1]
    capacity = top * tokens // experts
    wide_ref[...] = back_ref[...].astype(F32)
    expert = lax.broadcasted_iota(jnp.int32, (tokens, experts), 1)
    named = jnp.zeros((tokens, experts), F32)
    weighted = jnp.zeros((tokens, experts), F32)
    for k in range(top):
        hit = ids_ref[:, k : k + 1] == expert
        named += hit.astype(F32)
        weighted += jnp.where(hit, weights_ref[:, k : k + 1], 0.0)
    earlier = lax.broadcasted_iota(jnp.int32, (tokens, tokens), 1) < lax.broadcasted_iota(
        jnp.int32, (tokens, tokens), 0
    )
    rank = mm(earlier.astype(BF16), named.astype(BF16))
    moe_sum = 0.0
    for j in range(capacity):
        pick = jnp.where((named > 0.5) & (jnp.abs(rank - j) < 0.5), weighted, 0.0)
        for c in range(tiles):
            rows_ref[:, c * LANES : (c + 1) * LANES] = wide_ref[
                pl.ds(j * tiles + c, experts, stride=capacity * tiles), :
            ].astype(BF16)
        high = pick.astype(BF16)
        low = pick - high.astype(F32)
        middle = low.astype(BF16)
        last = (low - middle.astype(F32)).astype(BF16)
        rows = rows_ref[...]
        moe_sum = moe_sum + (mm(high, rows) + (mm(middle, rows) + mm(last, rows)))
    pre_final = RESIDUAL_SCALE * normed_ref[...].astype(F32) + moe_sum
    out_ref[...] = layer_norm(pre_final, gain_ref[...], bias_ref[...]).astype(BF16)


def per_device(
    resid,
    queries,
    keys,
    values,
    doc_ids,
    sink_logits,
    out_proj,
    norm1_gain,
    norm1_bias,
    route_ids,
    route_weights,
    expert_gate,
    expert_up,
    expert_down,
    norm2_gain,
    norm2_bias,
):
    tokens = queries.shape[0]
    own, width = resid.shape
    blocks, members = lax.axis_size("sp"), lax.axis_size("tp")
    experts = blocks
    capacity = route_ids.shape[1] * own // experts
    tiles = width // LANES
    packed = experts * capacity * tiles

    small = (keys.T, values.T, doc_ids.reshape(1, tokens), queries, out_proj, resid, sink_logits.reshape(1, -1))
    pack = shape((2 * HEAD_DIM + 16, WINDOW), BF16)
    keys_t, values_t, docs, queries, out_proj, resid, sinks, head, tail = call(
        functools.partial(first_body, len(small)),
        [shape(a.shape, a.dtype) for a in small] + [pack, pack],
        *[pltpu.with_memory_space_constraint(a, pltpu.HBM) for a in small],
        flops=10**5,
        specs=[HBM] * len(small),
        scratch=[pltpu.SemaphoreType.DMA((len(small),))],
    )
    previous = lax.ppermute(tail, "sp", [(i, i + 1) for i in range(blocks - 1)])
    following = lax.ppermute(head, "sp", [(i + 1, i) for i in range(blocks - 1)])
    (partial,) = call(
        attention_body,
        [shape((tokens, width), BF16)],
        sinks,
        queries,
        keys_t,
        values_t,
        docs,
        previous,
        following,
        out_proj,
        flops=10**9,
        scratch=[pltpu.VMEM(queries.shape, BF16)],
    )
    parts = lax.all_to_all(partial.reshape(members, own, width), "tp", 0, 0, tiled=True)
    normed, sent = call(
        functools.partial(dispatch_body, experts),
        [shape((own, width), BF16), shape((packed, LANES), BF16)],
        parts,
        resid,
        norm1_gain.reshape(1, -1),
        norm1_bias.reshape(1, -1),
        route_ids.T,
        flops=10**9,
        scratch=[pltpu.VMEM((packed, LANES), F32)],
    )
    arrived = lax.all_to_all(sent, "sp", 0, 0, tiled=True)

    def turned(array, by):
        return lax.ppermute(array, "tp", [(i, (i + by) % members) for i in range(members)])

    def expert_call(*row_sets):
        count, rows = len(row_sets), row_sets[0].shape[0]
        return call(
            functools.partial(expert_body, count),
            [shape((rows, LANES), BF16)] * count,
            *row_sets,
            expert_gate[0],
            expert_up[0],
            expert_down[0],
            flops=count * rows * 10**6,
            scratch=[
                pltpu.VMEM((count * rows // tiles, width), BF16),
                pltpu.VMEM((count, rows, LANES), F32),
            ],
        )

    half = packed // 2
    first, second = arrived[:half], arrived[half:]
    left_1, right_2 = turned(first, 1), turned(second, -1)
    left_2, right_1 = turned(second, 1), turned(first, -1)
    far_1, far_2 = turned(left_1, 1), turned(right_2, -1)
    (kept,) = expert_call(arrived)
    for_left_1, for_left_2, for_right_1, for_right_2 = expert_call(left_1, left_2, right_1, right_2)
    for_far_1, for_far_2 = expert_call(far_1, far_2)
    from_right_2 = turned(for_left_2, -1)
    from_left_1 = turned(for_right_1, 1)
    for_left_1 = for_left_1.astype(F32) + turned(for_far_1, -1).astype(F32)
    for_right_2 = for_right_2.astype(F32) + turned(for_far_2, 1).astype(F32)
    from_right_1 = turned(for_left_1.astype(BF16), -1)
    from_left_2 = turned(for_right_2.astype(BF16), 1)
    (summed,) = call(
        total_body,
        [shape((packed, LANES), BF16)],
        kept,
        from_left_1,
        from_right_1,
        from_left_2,
        from_right_2,
        flops=10**7,
    )
    back = lax.all_to_all(summed, "sp", 0, 0, tiled=True)
    (mixed,) = call(
        functools.partial(combine_body, experts),
        [shape((own, width), BF16)],
        back,
        normed,
        route_ids,
        route_weights,
        norm2_gain.reshape(1, -1),
        norm2_bias.reshape(1, -1),
        flops=10**9,
        scratch=[pltpu.VMEM((packed, LANES), F32), pltpu.VMEM((experts, width), BF16)],
    )
    return mixed


def solution(mesh):
    every = ("grp", "sp", "tp")
    group = ("grp", "sp")
    placed = (
        P(every, None),
        P(group, "tp"),
        P(group, "tp"),
        P(group, "tp"),
        P(group),
        P("tp"),
        P("tp", None),
        P(),
        P(),
        P(every, None),
        P(every, None),
        P("sp", None, "tp"),
        P("sp", None, "tp"),
        P("sp", "tp", None),
        P(),
        P(),
    )

    return jax.shard_map(
        per_device, mesh=mesh, in_specs=placed, out_specs=P(every, None), check_vma=False
    )
```

```python
import functools

import jax
import jax.numpy as jnp
from jax import lax
from jax.experimental import pallas as pl
from jax.experimental.pallas import tpu as pltpu
from jax.sharding import Mesh
from jax.sharding import PartitionSpec as P


HEAD_DIM = 64
WINDOW = 128
LANES = 128
NORM_EPSILON = 1e-05
RESIDUAL_SCALE = 1.4142135623730951
MASKED = -1e30
SP = ("chip", "core")
F32 = jnp.float32
BF16 = jnp.bfloat16


VMEM = pl.BlockSpec(memory_space=pltpu.VMEM)
HBM = pl.BlockSpec(memory_space=pltpu.HBM)


def mm(a, b):
    return jnp.dot(a, b, preferred_element_type=F32)


def mm_nt(a, b):
    return lax.dot_general(a, b, (((1,), (1,)), ((), ())), preferred_element_type=F32)


def mm_tn(a, b):
    return lax.dot_general(a, b, (((0,), (0,)), ((), ())), preferred_element_type=F32)


def call(body, out_shapes, *args, flops, specs=None, scratch=(), vmem=None):
    size = sum(a.size * a.dtype.itemsize for a in args)
    size += sum(s.size * s.dtype.itemsize for s in out_shapes)
    return pl.pallas_call(
        body,
        out_shape=out_shapes,
        in_specs=specs or [VMEM] * len(args),
        out_specs=[VMEM] * len(out_shapes),
        scratch_shapes=list(scratch),
        compiler_params=pltpu.CompilerParams(vmem_limit_bytes=vmem or 12 * 2**20),
        cost_estimate=pl.CostEstimate(flops=flops, bytes_accessed=size, transcendentals=0),
    )(*args)


def shape(dims, dtype):
    return jax.ShapeDtypeStruct(dims, dtype)


def layer_norm(values, gain, bias):
    centred = values - jnp.mean(values, -1, keepdims=True)
    variance = jnp.mean(centred * centred, -1, keepdims=True)
    return centred * lax.rsqrt(variance + NORM_EPSILON) * gain + bias


def first_body(count, core_ref, *refs):
    sources, held, (head_ref, tail_ref, core_out_ref, sems) = refs[:count], refs[count : 2 * count], refs[2 * count :]
    copies = [pltpu.make_async_copy(a, b, sems.at[i]) for i, (a, b) in enumerate(zip(sources, held))]
    for copy in copies:
        copy.start()
    core_out_ref[...] = core_ref[...]
    for copy in copies[:3]:
        copy.wait()
    keys_ref, values_ref, docs_ref = held[:3]
    tokens = keys_ref.shape[1]
    docs = (docs_ref[...].astype(F32) + 1.0).astype(BF16)
    for ref, lo in ((head_ref, 0), (tail_ref, tokens - WINDOW)):
        cols = slice(lo, lo + WINDOW)
        ref[0:HEAD_DIM, :] = keys_ref[:, cols]
        ref[HEAD_DIM : 2 * HEAD_DIM, :] = values_ref[:, cols]
        ref[2 * HEAD_DIM :, :] = jnp.broadcast_to(docs[:, cols], (16, WINDOW))
    for copy in copies[3:]:
        copy.wait()


def attention_body(
    sink_ref, query_ref, keys_ref, values_ref, docs_ref, prev_ref, next_ref, proj_ref, out_ref, att_ref
):
    tokens = query_ref.shape[0]
    heads = query_ref.shape[1] // HEAD_DIM
    own_docs = docs_ref[...].astype(F32) + 1.0
    query_docs = jnp.broadcast_to(own_docs, (LANES, tokens)).T[:, 0:1]
    row = lax.broadcasted_iota(jnp.int32, (tokens, 1), 0)
    blocks = []
    for key, value, docs, first in (
        (prev_ref[0:HEAD_DIM, :], prev_ref[HEAD_DIM : 2 * HEAD_DIM, :], None, -WINDOW),
        (keys_ref[...], values_ref[...], own_docs, 0),
        (next_ref[0:HEAD_DIM, :], next_ref[HEAD_DIM : 2 * HEAD_DIM, :], None, tokens),
    ):
        if docs is None:
            ref = prev_ref if first < 0 else next_ref
            docs = ref[2 * HEAD_DIM :, :].astype(F32)[0:1, :]
        width = key.shape[1]
        place = first + lax.broadcasted_iota(jnp.int32, (1, width), 1)
        allowed = (jnp.abs(row - place) <= WINDOW) & (query_docs == docs)
        blocks.append((key, value, allowed))
    for h in range(heads):
        cols = slice(h * HEAD_DIM, (h + 1) * HEAD_DIM)
        query = query_ref[:, cols]
        sink = sink_ref[:, h : h + 1]
        scores = [
            jnp.where(allowed, mm(query, key) * HEAD_DIM ** (-0.5), MASKED)
            for key, _, allowed in blocks
        ]
        top = functools.reduce(jnp.maximum, [jnp.max(s, -1, keepdims=True) for s in scores])
        top = jnp.maximum(top, sink)
        raised = [
            jnp.where(allowed, jnp.exp(s - top), 0.0) for s, (_, _, allowed) in zip(scores, blocks)
        ]
        total = jnp.exp(sink - top) + sum(jnp.sum(r, -1, keepdims=True) for r in raised)
        scale = 1.0 / total
        result = sum(
            mm_nt((r * scale).astype(BF16), value) for r, (_, value, _) in zip(raised, blocks)
        )
        att_ref[:, cols] = result.astype(BF16)
    out_ref[...] = mm(att_ref[...], proj_ref[...]).astype(BF16)


def routing_rows(ids, expert, weights=None):
    experts, tokens = expert.shape
    named = jnp.zeros((experts, tokens), F32)
    weighted = jnp.zeros((experts, tokens), F32)
    for k in range(ids.shape[0]):
        hit = ids[k : k + 1, :] == expert
        named += hit.astype(F32)
        if weights is not None:
            weighted += jnp.where(hit, weights[k : k + 1, :], 0.0)
    before = lax.broadcasted_iota(jnp.int32, (tokens, tokens), 0) < lax.broadcasted_iota(
        jnp.int32, (tokens, tokens), 1
    )
    rank = jnp.where(named > 0.5, mm(named.astype(BF16), before.astype(BF16)), -1.0)
    return (named if weights is None else weighted), rank


def dispatch_body(
    experts,
    parts_ref,
    resid_ref,
    gain_ref,
    bias_ref,
    ids_ref,
    core_ref,
    normed_ref,
    same_ref,
    other_ref,
    wide_ref,
):
    tokens, width = resid_ref.shape
    tiles = width // LANES
    capacity = ids_ref.shape[0] * tokens // experts
    projected = sum(parts_ref[i].astype(F32) for i in range(parts_ref.shape[0]))
    pre_norm = RESIDUAL_SCALE * resid_ref[...].astype(F32) + projected.astype(BF16).astype(F32)
    normed = layer_norm(pre_norm, gain_ref[...], bias_ref[...]).astype(BF16)
    normed_ref[...] = normed
    chips = experts // 2
    row = lax.broadcasted_iota(jnp.int32, (experts, tokens), 0)
    core = jnp.broadcast_to(core_ref[:, 0:1], (experts, tokens))
    expert = jnp.where(row < chips, 2 * row + core, 2 * (row - chips) + 1 - core)
    named, rank = routing_rows(ids_ref[...], expert)
    for j in range(capacity):
        pick = jnp.where(jnp.abs(rank - j) < 0.5, named, 0.0).astype(BF16)
        rows = mm(pick, normed)
        for c in range(tiles):
            wide_ref[pl.ds(j * tiles + c, experts, stride=capacity * tiles), :] = rows[
                :, c * LANES : (c + 1) * LANES
            ]
    half = same_ref.shape[0]
    same_ref[...] = wide_ref[0:half, :].astype(BF16)
    other_ref[...] = wide_ref[half:, :].astype(BF16)


def pair_body(same_ref, other_ref, core_ref, out_ref):
    per_expert = same_ref.shape[1]
    first_core = jnp.broadcast_to(core_ref[...], same_ref.shape) == 0
    same, other = same_ref[...].astype(F32), other_ref[...].astype(F32)
    out_ref[:, 0:per_expert, :] = jnp.where(first_core, same, other).astype(BF16)
    out_ref[:, per_expert:, :] = jnp.where(first_core, other, same).astype(BF16)


def expert_body(count, *refs):
    row_refs, (gate_ref, up_ref, down_ref), refs = refs[:count], refs[count : count + 3], refs[count + 3 :]
    out_refs, (lhs, wide) = refs[:count], refs[count:]
    tiles = gate_ref.shape[0] // LANES
    rows = row_refs[0].shape[0] // tiles
    for b, ref in enumerate(row_refs):
        wide[b] = ref[...].astype(F32)
        for c in range(tiles):
            lhs[b * rows : (b + 1) * rows, c * LANES : (c + 1) * LANES] = wide.at[b][
                pl.ds(c, rows, stride=tiles), :
            ].astype(BF16)
    gate_act = mm(lhs[...], gate_ref[...])
    up_act = mm(lhs[...], up_ref[...])
    act = (gate_act / (1.0 + jnp.exp(-gate_act)) * up_act).astype(BF16)
    step = 4 * LANES
    for i in range(0, down_ref.shape[1], step):
        result = mm(act, down_ref[:, i : i + step])
        for t in range(0, step, LANES):
            for b in range(count):
                wide.at[b][pl.ds((i + t) // LANES, rows, stride=tiles), :] = result[
                    b * rows : (b + 1) * rows, t : t + LANES
                ]
    for b in range(count):
        out_refs[b][...] = wide[b].astype(BF16)


def total_body(kept_ref, left_1_ref, right_1_ref, left_2_ref, right_2_ref, out_ref):
    half = left_1_ref.shape[0]
    for part, left_ref, right_ref in ((0, left_1_ref, right_1_ref), (1, left_2_ref, right_2_ref)):
        rows = slice(part * half, (part + 1) * half)
        sides = left_ref[...].astype(F32) + right_ref[...].astype(F32)
        out_ref[rows, :] = (kept_ref[rows, :].astype(F32) + sides).astype(BF16)


def combine_body(
    experts, back_ref, normed_ref, ids_ref, weights_ref, gain_ref, bias_ref, out_ref, wide_ref, rows_ref
):
    tokens, width = normed_ref.shape
    tiles = width // LANES
    capacity = ids_ref.shape[0] * tokens // experts
    wide_ref[...] = back_ref[...].astype(F32)
    expert = lax.broadcasted_iota(jnp.int32, (experts, tokens), 0)
    weighted, rank = routing_rows(ids_ref[...], expert, weights_ref[...])
    moe_sum = 0.0
    for j in range(capacity):
        pick = jnp.where(jnp.abs(rank - j) < 0.5, weighted, 0.0)
        for c in range(tiles):
            rows_ref[:, c * LANES : (c + 1) * LANES] = wide_ref[
                pl.ds(j * tiles + c, experts, stride=capacity * tiles), :
            ].astype(BF16)
        high = pick.astype(BF16)
        low = pick - high.astype(F32)
        middle = low.astype(BF16)
        last = (low - middle.astype(F32)).astype(BF16)
        rows = rows_ref[...]
        moe_sum = moe_sum + (mm_tn(high, rows) + (mm_tn(middle, rows) + mm_tn(last, rows)))
    pre_final = RESIDUAL_SCALE * normed_ref[...].astype(F32) + moe_sum
    out_ref[...] = layer_norm(pre_final, gain_ref[...], bias_ref[...]).astype(BF16)


def per_device(
    resid,
    queries,
    keys,
    values,
    doc_ids,
    sink_logits,
    out_proj,
    norm1_gain,
    norm1_bias,
    route_ids,
    route_weights,
    expert_gate,
    expert_up,
    expert_down,
    norm2_gain,
    norm2_bias,
):
    tokens = queries.shape[0]
    own, width = resid.shape
    blocks, members = lax.axis_size(SP), lax.axis_size("tp")
    experts = blocks
    capacity = route_ids.shape[1] * own // experts
    tiles = width // LANES
    packed = experts * capacity * tiles

    small = (keys.T, values.T, doc_ids.reshape(1, tokens), queries, out_proj, resid, sink_logits.reshape(1, -1))
    pack = shape((2 * HEAD_DIM + 16, WINDOW), BF16)
    core = jnp.full((1, LANES), lax.axis_index("core"), jnp.int32)
    keys_t, values_t, docs, queries, out_proj, resid, sinks, head, tail, core = call(
        functools.partial(first_body, len(small)),
        [shape(a.shape, a.dtype) for a in small] + [pack, pack, shape(core.shape, core.dtype)],
        core,
        *[pltpu.with_memory_space_constraint(a, pltpu.HBM) for a in small],
        flops=10**5,
        specs=[VMEM] + [HBM] * len(small),
        scratch=[pltpu.SemaphoreType.DMA((len(small),))],
    )
    previous = lax.ppermute(tail, SP, [(i, i + 1) for i in range(blocks - 1)])
    following = lax.ppermute(head, SP, [(i + 1, i) for i in range(blocks - 1)])
    (partial,) = call(
        attention_body,
        [shape((tokens, width), BF16)],
        sinks,
        queries,
        keys_t,
        values_t,
        docs,
        previous,
        following,
        out_proj,
        flops=10**9,
        scratch=[pltpu.VMEM(queries.shape, BF16)],
    )
    parts = lax.all_to_all(partial.reshape(members, own, width), "tp", 0, 0, tiled=True)
    normed, same, other = call(
        functools.partial(dispatch_body, experts),
        [shape((own, width), BF16)] + [shape((packed // 2, LANES), BF16)] * 2,
        parts,
        resid,
        norm1_gain.reshape(1, -1),
        norm1_bias.reshape(1, -1),
        route_ids.T,
        core,
        flops=10**9,
        scratch=[pltpu.VMEM((packed, LANES), F32)],
    )
    other = lax.ppermute(other, "core", [(0, 1), (1, 0)])
    per_expert = capacity * tiles
    (sent,) = call(
        pair_body,
        [shape((experts // 2, 2 * per_expert, LANES), BF16)],
        same.reshape(-1, per_expert, LANES),
        other.reshape(-1, per_expert, LANES),
        core,
        flops=10**6,
    )
    arrived = lax.all_to_all(sent.reshape(packed, LANES), "chip", 0, 0, tiled=True)

    def turned(array, by):
        return lax.ppermute(array, "tp", [(i, (i + by) % members) for i in range(members)])

    def expert_call(*row_sets):
        count, rows = len(row_sets), row_sets[0].shape[0]
        return call(
            functools.partial(expert_body, count),
            [shape((rows, LANES), BF16)] * count,
            *row_sets,
            expert_gate[0],
            expert_up[0],
            expert_down[0],
            flops=count * rows * 10**6,
            scratch=[
                pltpu.VMEM((count * rows // tiles, width), BF16),
                pltpu.VMEM((count, rows, LANES), F32),
            ],
        )

    half = packed // 2
    first, second = arrived[:half], arrived[half:]
    left_1, right_2 = turned(first, 1), turned(second, -1)
    left_2, right_1 = turned(second, 1), turned(first, -1)
    far_1, far_2 = turned(left_1, 1), turned(right_2, -1)
    (kept,) = expert_call(arrived)
    for_left_1, for_left_2, for_right_1, for_right_2 = expert_call(left_1, left_2, right_1, right_2)
    for_far_1, for_far_2 = expert_call(far_1, far_2)
    from_right_2 = turned(for_left_2, -1)
    from_left_1 = turned(for_right_1, 1)
    for_left_1 = for_left_1.astype(F32) + turned(for_far_1, -1).astype(F32)
    for_right_2 = for_right_2.astype(F32) + turned(for_far_2, 1).astype(F32)
    from_right_1 = turned(for_left_1.astype(BF16), -1)
    from_left_2 = turned(for_right_2.astype(BF16), 1)
    (summed,) = call(
        total_body,
        [shape((packed, LANES), BF16)],
        kept,
        from_left_1,
        from_right_1,
        from_left_2,
        from_right_2,
        flops=10**7,
    )
    back = lax.all_to_all(summed, SP, 0, 0, tiled=True)
    (mixed,) = call(
        functools.partial(combine_body, experts),
        [shape((own, width), BF16)],
        back,
        normed,
        route_ids.T,
        route_weights.T,
        norm2_gain.reshape(1, -1),
        norm2_bias.reshape(1, -1),
        flops=10**9,
        scratch=[pltpu.VMEM((packed, LANES), F32), pltpu.VMEM((experts, width), BF16)],
    )
    return mixed


def solution(mesh):
    groups, cores = mesh.shape["grp"], 2
    chips = mesh.shape["sp"] // cores
    devices = mesh.devices.reshape(groups, chips, cores, mesh.shape["tp"])
    mesh = Mesh(devices, ("grp", *SP, "tp"))
    every = ("grp", *SP, "tp")
    group = ("grp", *SP)
    placed = (
        P(every, None),
        P(group, "tp"),
        P(group, "tp"),
        P(group, "tp"),
        P(group),
        P("tp"),
        P("tp", None),
        P(),
        P(),
        P(every, None),
        P(every, None),
        P(SP, None, "tp"),
        P(SP, None, "tp"),
        P(SP, "tp", None),
        P(),
        P(),
    )

    return jax.shard_map(
        per_device, mesh=mesh, in_specs=placed, out_specs=P(every, None), check_vma=False
    )
```

```python
import functools

import jax
import jax.numpy as jnp
from jax import lax
from jax.experimental import pallas as pl
from jax.experimental.pallas import tpu as pltpu
from jax.sharding import Mesh
from jax.sharding import PartitionSpec as P


HEAD_DIM = 64
WINDOW = 128
LANES = 128
NORM_EPSILON = 1e-05
RESIDUAL_SCALE = 1.4142135623730951
MASKED = -1e30
SP = ("chip", "core")
F32 = jnp.float32
BF16 = jnp.bfloat16


VMEM = pl.BlockSpec(memory_space=pltpu.VMEM)
HBM = pl.BlockSpec(memory_space=pltpu.HBM)


def mm(a, b):
    return jnp.dot(a, b, preferred_element_type=F32)


def mm_nt(a, b):
    return lax.dot_general(a, b, (((1,), (1,)), ((), ())), preferred_element_type=F32)


def mm_tn(a, b):
    return lax.dot_general(a, b, (((0,), (0,)), ((), ())), preferred_element_type=F32)


def call(body, out_shapes, *args, flops, specs=None, scratch=(), vmem=None):
    size = sum(a.size * a.dtype.itemsize for a in args)
    size += sum(s.size * s.dtype.itemsize for s in out_shapes)
    return pl.pallas_call(
        body,
        out_shape=out_shapes,
        in_specs=specs or [VMEM] * len(args),
        out_specs=[VMEM] * len(out_shapes),
        scratch_shapes=list(scratch),
        compiler_params=pltpu.CompilerParams(vmem_limit_bytes=vmem or 12 * 2**20),
        cost_estimate=pl.CostEstimate(flops=flops, bytes_accessed=size, transcendentals=0),
    )(*args)


def shape(dims, dtype):
    return jax.ShapeDtypeStruct(dims, dtype)


def layer_norm(values, gain, bias):
    centred = values - jnp.mean(values, -1, keepdims=True)
    variance = jnp.mean(centred * centred, -1, keepdims=True)
    return centred * lax.rsqrt(variance + NORM_EPSILON) * gain + bias


def first_body(count, core_ref, *refs):
    sources, held, (head_ref, tail_ref, core_out_ref, sems) = refs[:count], refs[count : 2 * count], refs[2 * count :]
    copies = [pltpu.make_async_copy(a, b, sems.at[i]) for i, (a, b) in enumerate(zip(sources, held))]
    for copy in copies:
        copy.start()
    core_out_ref[...] = core_ref[...]
    for copy in copies[:3]:
        copy.wait()
    keys_ref, values_ref, docs_ref = held[:3]
    tokens = keys_ref.shape[1]
    docs = (docs_ref[...].astype(F32) + 1.0).astype(BF16)
    for ref, lo in ((head_ref, 0), (tail_ref, tokens - WINDOW)):
        cols = slice(lo, lo + WINDOW)
        ref[0:HEAD_DIM, :] = keys_ref[:, cols]
        ref[HEAD_DIM : 2 * HEAD_DIM, :] = values_ref[:, cols]
        ref[2 * HEAD_DIM :, :] = jnp.broadcast_to(docs[:, cols], (16, WINDOW))
    for copy in copies[3:]:
        copy.wait()


def attention_body(
    sink_ref, query_ref, keys_ref, values_ref, docs_ref, prev_ref, next_ref, proj_ref, out_ref, att_ref
):
    tokens = query_ref.shape[0]
    heads = query_ref.shape[1] // HEAD_DIM
    own_docs = docs_ref[...].astype(F32) + 1.0
    query_docs = jnp.broadcast_to(own_docs, (LANES, tokens)).T[:, 0:1]
    row = lax.broadcasted_iota(jnp.int32, (tokens, 1), 0)
    blocks = []
    for key, value, docs, first in (
        (prev_ref[0:HEAD_DIM, :], prev_ref[HEAD_DIM : 2 * HEAD_DIM, :], None, -WINDOW),
        (keys_ref[...], values_ref[...], own_docs, 0),
        (next_ref[0:HEAD_DIM, :], next_ref[HEAD_DIM : 2 * HEAD_DIM, :], None, tokens),
    ):
        if docs is None:
            ref = prev_ref if first < 0 else next_ref
            docs = ref[2 * HEAD_DIM :, :].astype(F32)[0:1, :]
        width = key.shape[1]
        place = first + lax.broadcasted_iota(jnp.int32, (1, width), 1)
        allowed = (jnp.abs(row - place) <= WINDOW) & (query_docs == docs)
        blocks.append((key, value, allowed))
    for h in range(heads):
        cols = slice(h * HEAD_DIM, (h + 1) * HEAD_DIM)
        query = query_ref[:, cols]
        sink = sink_ref[:, h : h + 1]
        scores = [
            jnp.where(allowed, mm(query, key) * HEAD_DIM ** (-0.5), MASKED)
            for key, _, allowed in blocks
        ]
        top = functools.reduce(jnp.maximum, [jnp.max(s, -1, keepdims=True) for s in scores])
        top = jnp.maximum(top, sink)
        raised = [
            jnp.where(allowed, jnp.exp(s - top), 0.0) for s, (_, _, allowed) in zip(scores, blocks)
        ]
        total = jnp.exp(sink - top) + sum(jnp.sum(r, -1, keepdims=True) for r in raised)
        scale = 1.0 / total
        result = sum(
            mm_nt((r * scale).astype(BF16), value) for r, (_, value, _) in zip(raised, blocks)
        )
        att_ref[:, cols] = result.astype(BF16)
    out_ref[...] = mm(att_ref[...], proj_ref[...]).astype(BF16)


def routing_rows(ids, expert, weights=None):
    experts, tokens = expert.shape
    named = jnp.zeros((experts, tokens), F32)
    weighted = jnp.zeros((experts, tokens), F32)
    for k in range(ids.shape[0]):
        hit = ids[k : k + 1, :] == expert
        named += hit.astype(F32)
        if weights is not None:
            weighted += jnp.where(hit, weights[k : k + 1, :], 0.0)
    before = lax.broadcasted_iota(jnp.int32, (tokens, tokens), 0) < lax.broadcasted_iota(
        jnp.int32, (tokens, tokens), 1
    )
    rank = jnp.where(named > 0.5, mm(named.astype(BF16), before.astype(BF16)), -1.0)
    return (named if weights is None else weighted), rank


def dispatch_body(
    experts,
    parts_ref,
    resid_ref,
    gain_ref,
    bias_ref,
    ids_ref,
    core_ref,
    normed_ref,
    same_ref,
    other_ref,
    wide_ref,
):
    tokens, width = resid_ref.shape
    tiles = width // LANES
    capacity = ids_ref.shape[0] * tokens // experts
    projected = sum(parts_ref[i].astype(F32) for i in range(parts_ref.shape[0]))
    pre_norm = RESIDUAL_SCALE * resid_ref[...].astype(F32) + projected.astype(BF16).astype(F32)
    normed = layer_norm(pre_norm, gain_ref[...], bias_ref[...]).astype(BF16)
    normed_ref[...] = normed
    chips = experts // 2
    row = lax.broadcasted_iota(jnp.int32, (experts, tokens), 0)
    core = jnp.broadcast_to(core_ref[:, 0:1], (experts, tokens))
    expert = jnp.where(row < chips, 2 * row + core, 2 * (row - chips) + 1 - core)
    named, rank = routing_rows(ids_ref[...], expert)
    for j in range(capacity):
        pick = jnp.where(jnp.abs(rank - j) < 0.5, named, 0.0).astype(BF16)
        rows = mm(pick, normed)
        for c in range(tiles):
            wide_ref[pl.ds(j * tiles + c, experts, stride=capacity * tiles), :] = rows[
                :, c * LANES : (c + 1) * LANES
            ]
    half = same_ref.shape[0]
    same_ref[...] = wide_ref[0:half, :].astype(BF16)
    other_ref[...] = wide_ref[half:, :].astype(BF16)


def pair_body(same_ref, other_ref, core_ref, out_ref):
    per_expert = same_ref.shape[1]
    first_core = jnp.broadcast_to(core_ref[...], same_ref.shape) == 0
    same, other = same_ref[...].astype(F32), other_ref[...].astype(F32)
    out_ref[:, 0:per_expert, :] = jnp.where(first_core, same, other).astype(BF16)
    out_ref[:, per_expert:, :] = jnp.where(first_core, other, same).astype(BF16)


def expert_body(count, *refs):
    row_refs, (gate_ref, up_ref, down_ref), refs = refs[:count], refs[count : count + 3], refs[count + 3 :]
    out_refs, (lhs, wide) = refs[:count], refs[count:]
    tiles = gate_ref.shape[0] // LANES
    rows = row_refs[0].shape[0] // tiles
    for b, ref in enumerate(row_refs):
        wide[b] = ref[...].astype(F32)
        for c in range(tiles):
            lhs[b * rows : (b + 1) * rows, c * LANES : (c + 1) * LANES] = wide.at[b][
                pl.ds(c, rows, stride=tiles), :
            ].astype(BF16)
    gate_act = mm(lhs[...], gate_ref[...])
    up_act = mm(lhs[...], up_ref[...])
    act = (gate_act / (1.0 + jnp.exp(-gate_act)) * up_act).astype(BF16)
    step = 4 * LANES
    for i in range(0, down_ref.shape[1], step):
        result = mm(act, down_ref[:, i : i + step])
        for t in range(0, step, LANES):
            for b in range(count):
                wide.at[b][pl.ds((i + t) // LANES, rows, stride=tiles), :] = result[
                    b * rows : (b + 1) * rows, t : t + LANES
                ]
    for b in range(count):
        out_refs[b][...] = wide[b].astype(BF16)


def total_body(
    kept_ref, left_1_ref, right_1_ref, left_2_ref, right_2_ref, core_ref, same_ref, other_ref
):
    chips, per_expert, _ = same_ref.shape
    half = chips // 2
    first_core = jnp.broadcast_to(core_ref[...], (half, per_expert, LANES)) == 0
    for part, left_ref, right_ref in ((0, left_1_ref, right_1_ref), (1, left_2_ref, right_2_ref)):
        rows = slice(part * half, (part + 1) * half)
        sides = left_ref[...].astype(F32) + right_ref[...].astype(F32)
        result = kept_ref[rows].astype(F32) + sides
        zero, one = result[:, 0:per_expert, :], result[:, per_expert:, :]
        same_ref[rows] = jnp.where(first_core, zero, one).astype(BF16)
        other_ref[rows] = jnp.where(first_core, one, zero).astype(BF16)


def combine_body(
    experts, back_ref, normed_ref, ids_ref, weights_ref, gain_ref, bias_ref, out_ref, wide_ref, rows_ref
):
    tokens, width = normed_ref.shape
    tiles = width // LANES
    capacity = ids_ref.shape[0] * tokens // experts
    wide_ref[...] = back_ref[...].astype(F32)
    expert = lax.broadcasted_iota(jnp.int32, (experts, tokens), 0)
    weighted, rank = routing_rows(ids_ref[...], expert, weights_ref[...])
    moe_sum = 0.0
    for j in range(capacity):
        pick = jnp.where(jnp.abs(rank - j) < 0.5, weighted, 0.0)
        for c in range(tiles):
            rows_ref[:, c * LANES : (c + 1) * LANES] = wide_ref[
                pl.ds(j * tiles + c, experts, stride=capacity * tiles), :
            ].astype(BF16)
        high = pick.astype(BF16)
        low = pick - high.astype(F32)
        middle = low.astype(BF16)
        last = (low - middle.astype(F32)).astype(BF16)
        rows = rows_ref[...]
        moe_sum = moe_sum + (mm_tn(high, rows) + (mm_tn(middle, rows) + mm_tn(last, rows)))
    pre_final = RESIDUAL_SCALE * normed_ref[...].astype(F32) + moe_sum
    out_ref[...] = layer_norm(pre_final, gain_ref[...], bias_ref[...]).astype(BF16)


def per_device(
    resid,
    queries,
    keys,
    values,
    doc_ids,
    sink_logits,
    out_proj,
    norm1_gain,
    norm1_bias,
    route_ids,
    route_weights,
    expert_gate,
    expert_up,
    expert_down,
    norm2_gain,
    norm2_bias,
):
    tokens = queries.shape[0]
    own, width = resid.shape
    blocks, members = lax.axis_size(SP), lax.axis_size("tp")
    experts = blocks
    capacity = route_ids.shape[1] * own // experts
    tiles = width // LANES
    packed = experts * capacity * tiles

    small = (keys.T, values.T, doc_ids.reshape(1, tokens), queries, out_proj, resid, sink_logits.reshape(1, -1))
    pack = shape((2 * HEAD_DIM + 16, WINDOW), BF16)
    core = jnp.full((1, LANES), lax.axis_index("core"), jnp.int32)
    keys_t, values_t, docs, queries, out_proj, resid, sinks, head, tail, core = call(
        functools.partial(first_body, len(small)),
        [shape(a.shape, a.dtype) for a in small] + [pack, pack, shape(core.shape, core.dtype)],
        core,
        *[pltpu.with_memory_space_constraint(a, pltpu.HBM) for a in small],
        flops=10**5,
        specs=[VMEM] + [HBM] * len(small),
        scratch=[pltpu.SemaphoreType.DMA((len(small),))],
    )
    previous = lax.ppermute(tail, SP, [(i, i + 1) for i in range(blocks - 1)])
    following = lax.ppermute(head, SP, [(i + 1, i) for i in range(blocks - 1)])
    (partial,) = call(
        attention_body,
        [shape((tokens, width), BF16)],
        sinks,
        queries,
        keys_t,
        values_t,
        docs,
        previous,
        following,
        out_proj,
        flops=10**9,
        scratch=[pltpu.VMEM(queries.shape, BF16)],
    )
    parts = lax.all_to_all(partial.reshape(members, own, width), "tp", 0, 0, tiled=True)
    normed, same, other = call(
        functools.partial(dispatch_body, experts),
        [shape((own, width), BF16)] + [shape((packed // 2, LANES), BF16)] * 2,
        parts,
        resid,
        norm1_gain.reshape(1, -1),
        norm1_bias.reshape(1, -1),
        route_ids.T,
        core,
        flops=10**9,
        scratch=[pltpu.VMEM((packed, LANES), F32)],
    )
    per_expert = capacity * tiles
    chips = experts // 2

    def exchanged(same, other):
        other = lax.ppermute(other, "core", [(0, 1), (1, 0)])
        (sent,) = call(
            pair_body,
            [shape((chips, 2 * per_expert, LANES), BF16)],
            same.reshape(chips, per_expert, LANES),
            other.reshape(chips, per_expert, LANES),
            core,
            flops=10**6,
        )
        return lax.all_to_all(sent.reshape(packed, LANES), "chip", 0, 0, tiled=True)

    arrived = exchanged(same, other)

    def turned(array, by):
        return lax.ppermute(array, "tp", [(i, (i + by) % members) for i in range(members)])

    def expert_call(*row_sets):
        count, rows = len(row_sets), row_sets[0].shape[0]
        return call(
            functools.partial(expert_body, count),
            [shape((rows, LANES), BF16)] * count,
            *row_sets,
            expert_gate[0],
            expert_up[0],
            expert_down[0],
            flops=count * rows * 10**6,
            scratch=[
                pltpu.VMEM((count * rows // tiles, width), BF16),
                pltpu.VMEM((count, rows, LANES), F32),
            ],
        )

    half = packed // 2
    first, second = arrived[:half], arrived[half:]
    left_1, right_2 = turned(first, 1), turned(second, -1)
    left_2, right_1 = turned(second, 1), turned(first, -1)
    far_1, far_2 = turned(left_1, 1), turned(right_2, -1)
    (kept,) = expert_call(arrived)
    for_left_1, for_left_2, for_right_1, for_right_2 = expert_call(left_1, left_2, right_1, right_2)
    for_far_1, for_far_2 = expert_call(far_1, far_2)
    from_right_2 = turned(for_left_2, -1)
    from_left_1 = turned(for_right_1, 1)
    for_left_1 = for_left_1.astype(F32) + turned(for_far_1, -1).astype(F32)
    for_right_2 = for_right_2.astype(F32) + turned(for_far_2, 1).astype(F32)
    from_right_1 = turned(for_left_1.astype(BF16), -1)
    from_left_2 = turned(for_right_2.astype(BF16), 1)
    sides = [from_left_1, from_right_1, from_left_2, from_right_2]
    same, other = call(
        total_body,
        [shape((chips, per_expert, LANES), BF16)] * 2,
        kept.reshape(chips, 2 * per_expert, LANES),
        *[side.reshape(chips // 2, 2 * per_expert, LANES) for side in sides],
        core,
        flops=10**7,
    )
    back = exchanged(same, other)
    (mixed,) = call(
        functools.partial(combine_body, experts),
        [shape((own, width), BF16)],
        back,
        normed,
        route_ids.T,
        route_weights.T,
        norm2_gain.reshape(1, -1),
        norm2_bias.reshape(1, -1),
        flops=10**9,
        scratch=[pltpu.VMEM((packed, LANES), F32), pltpu.VMEM((experts, width), BF16)],
    )
    return mixed


def solution(mesh):
    groups, cores = mesh.shape["grp"], 2
    chips = mesh.shape["sp"] // cores
    devices = mesh.devices.reshape(groups, chips, cores, mesh.shape["tp"])
    mesh = Mesh(devices, ("grp", *SP, "tp"))
    every = ("grp", *SP, "tp")
    group = ("grp", *SP)
    placed = (
        P(every, None),
        P(group, "tp"),
        P(group, "tp"),
        P(group, "tp"),
        P(group),
        P("tp"),
        P("tp", None),
        P(),
        P(),
        P(every, None),
        P(every, None),
        P(SP, None, "tp"),
        P(SP, None, "tp"),
        P(SP, "tp", None),
        P(),
        P(),
    )

    return jax.shard_map(per_device, mesh=mesh, in_specs=placed, out_specs=P(every, None), check_vma=False)
```

```python
import functools

import jax
import jax.numpy as jnp
from jax import lax
from jax.experimental import pallas as pl
from jax.experimental.pallas import tpu as pltpu
from jax.sharding import Mesh
from jax.sharding import PartitionSpec as P


HEAD_DIM = 64
WINDOW = 128
LANES = 128
NORM_EPSILON = 1e-05
RESIDUAL_SCALE = 1.4142135623730951
MASKED = -1e30
SP = ("chip", "core")
F32 = jnp.float32
BF16 = jnp.bfloat16


VMEM = pl.BlockSpec(memory_space=pltpu.VMEM)
HBM = pl.BlockSpec(memory_space=pltpu.HBM)


def mm(a, b):
    return jnp.dot(a, b, preferred_element_type=F32)


def mm_nt(a, b):
    return lax.dot_general(a, b, (((1,), (1,)), ((), ())), preferred_element_type=F32)


def mm_tn(a, b):
    return lax.dot_general(a, b, (((0,), (0,)), ((), ())), preferred_element_type=F32)


def call(body, out_shapes, *args, flops, specs=None, scratch=(), vmem=None):
    size = sum(a.size * a.dtype.itemsize for a in args)
    size += sum(s.size * s.dtype.itemsize for s in out_shapes)
    return pl.pallas_call(
        body,
        out_shape=out_shapes,
        in_specs=specs or [VMEM] * len(args),
        out_specs=[VMEM] * len(out_shapes),
        scratch_shapes=list(scratch),
        compiler_params=pltpu.CompilerParams(vmem_limit_bytes=vmem or 12 * 2**20),
        cost_estimate=pl.CostEstimate(flops=flops, bytes_accessed=size, transcendentals=0),
    )(*args)


def in_hbm(array):
    return pltpu.with_memory_space_constraint(array, pltpu.HBM)


def shape(dims, dtype):
    return jax.ShapeDtypeStruct(dims, dtype)


def layer_norm(values, gain, bias):
    centred = values - jnp.mean(values, -1, keepdims=True)
    variance = jnp.mean(centred * centred, -1, keepdims=True)
    return centred * lax.rsqrt(variance + NORM_EPSILON) * gain + bias


def first_body(count, core_ref, *refs):
    sources, held, (head_ref, tail_ref, core_out_ref, sems) = refs[:count], refs[count : 2 * count], refs[2 * count :]
    copies = [pltpu.make_async_copy(a, b, sems.at[i]) for i, (a, b) in enumerate(zip(sources, held))]
    for copy in copies:
        copy.start()
    core_out_ref[...] = core_ref[...]
    for copy in copies[:3]:
        copy.wait()
    keys_ref, values_ref, docs_ref = held[:3]
    tokens = keys_ref.shape[1]
    docs = (docs_ref[...].astype(F32) + 1.0).astype(BF16)
    for ref, lo in ((head_ref, 0), (tail_ref, tokens - WINDOW)):
        cols = slice(lo, lo + WINDOW)
        ref[0:HEAD_DIM, :] = keys_ref[:, cols]
        ref[HEAD_DIM : 2 * HEAD_DIM, :] = values_ref[:, cols]
        ref[2 * HEAD_DIM :, :] = jnp.broadcast_to(docs[:, cols], (16, WINDOW))
    for copy in copies[3:]:
        copy.wait()


def attention_body(
    sink_ref,
    query_ref,
    keys_ref,
    values_ref,
    docs_ref,
    prev_ref,
    next_ref,
    proj_hbm,
    resid_hbm,
    out_ref,
    resid_ref,
    att_ref,
    proj_ref,
    sems,
):
    proj_copy = pltpu.make_async_copy(proj_hbm, proj_ref, sems.at[0])
    resid_copy = pltpu.make_async_copy(resid_hbm, resid_ref, sems.at[1])
    proj_copy.start()
    resid_copy.start()
    tokens = query_ref.shape[0]
    heads = query_ref.shape[1] // HEAD_DIM
    own_docs = docs_ref[...].astype(F32) + 1.0
    query_docs = jnp.broadcast_to(own_docs, (LANES, tokens)).T[:, 0:1]
    row = lax.broadcasted_iota(jnp.int32, (tokens, 1), 0)
    blocks = []
    for key, value, docs, first in (
        (prev_ref[0:HEAD_DIM, :], prev_ref[HEAD_DIM : 2 * HEAD_DIM, :], None, -WINDOW),
        (keys_ref[...], values_ref[...], own_docs, 0),
        (next_ref[0:HEAD_DIM, :], next_ref[HEAD_DIM : 2 * HEAD_DIM, :], None, tokens),
    ):
        if docs is None:
            ref = prev_ref if first < 0 else next_ref
            docs = ref[2 * HEAD_DIM :, :].astype(F32)[0:1, :]
        width = key.shape[1]
        place = first + lax.broadcasted_iota(jnp.int32, (1, width), 1)
        allowed = (jnp.abs(row - place) <= WINDOW) & (query_docs == docs)
        blocks.append((key, value, jnp.where(allowed, 0.0, MASKED)))
    for h in range(heads):
        cols = slice(h * HEAD_DIM, (h + 1) * HEAD_DIM)
        query = query_ref[:, cols]
        sink = sink_ref[:, h : h + 1]
        scores = [
            mm(query, key) * HEAD_DIM ** (-0.5) + hidden for key, _, hidden in blocks
        ]
        top = functools.reduce(jnp.maximum, [jnp.max(s, -1, keepdims=True) for s in scores])
        top = jnp.maximum(top, sink)
        raised = [jnp.exp(s - top) for s in scores]
        total = jnp.exp(sink - top) + sum(jnp.sum(r, -1, keepdims=True) for r in raised)
        scale = 1.0 / total
        result = sum(
            mm_nt((r * scale).astype(BF16), value) for r, (_, value, _) in zip(raised, blocks)
        )
        att_ref[:, cols] = result.astype(BF16)
    proj_copy.wait()
    out_ref[...] = mm(att_ref[...], proj_ref[...]).astype(BF16)
    resid_copy.wait()


def routing_rows(ids, expert, weights=None):
    experts, tokens = expert.shape
    named = jnp.zeros((experts, tokens), F32)
    weighted = jnp.zeros((experts, tokens), F32)
    for k in range(ids.shape[0]):
        hit = ids[k : k + 1, :] == expert
        named += hit.astype(F32)
        if weights is not None:
            weighted += jnp.where(hit, weights[k : k + 1, :], 0.0)
    before = lax.broadcasted_iota(jnp.int32, (tokens, tokens), 0) < lax.broadcasted_iota(
        jnp.int32, (tokens, tokens), 1
    )
    rank = jnp.where(named > 0.5, mm(named.astype(BF16), before.astype(BF16)), -1.0)
    return (named if weights is None else weighted), rank


def dispatch_body(
    experts,
    parts_ref,
    resid_ref,
    gain_ref,
    bias_ref,
    ids_ref,
    core_ref,
    normed_ref,
    same_ref,
    other_ref,
    wide_ref,
):
    tokens, width = resid_ref.shape
    tiles = width // LANES
    capacity = ids_ref.shape[0] * tokens // experts
    projected = sum(parts_ref[i].astype(F32) for i in range(parts_ref.shape[0]))
    pre_norm = RESIDUAL_SCALE * resid_ref[...].astype(F32) + projected.astype(BF16).astype(F32)
    normed = layer_norm(pre_norm, gain_ref[...], bias_ref[...]).astype(BF16)
    normed_ref[...] = normed
    chips = experts // 2
    row = lax.broadcasted_iota(jnp.int32, (experts, tokens), 0)
    core = jnp.broadcast_to(core_ref[:, 0:1], (experts, tokens))
    expert = jnp.where(row < chips, 2 * row + core, 2 * (row - chips) + 1 - core)
    named, rank = routing_rows(ids_ref[...], expert)
    for j in range(capacity):
        pick = jnp.where(jnp.abs(rank - j) < 0.5, named, 0.0).astype(BF16)
        rows = mm(pick, normed)
        for c in range(tiles):
            wide_ref[pl.ds(j * tiles + c, experts, stride=capacity * tiles), :] = rows[
                :, c * LANES : (c + 1) * LANES
            ]
    half = same_ref.shape[0]
    same_ref[...] = wide_ref[0:half, :].astype(BF16)
    other_ref[...] = wide_ref[half:, :].astype(BF16)


def pair_body(same_ref, other_ref, core_ref, out_ref):
    per_expert = same_ref.shape[1]
    first_core = jnp.broadcast_to(core_ref[...], same_ref.shape) == 0
    same, other = same_ref[...].astype(F32), other_ref[...].astype(F32)
    out_ref[:, 0:per_expert, :] = jnp.where(first_core, same, other).astype(BF16)
    out_ref[:, per_expert:, :] = jnp.where(first_core, other, same).astype(BF16)


def expert_body(count, *refs):
    row_refs, (gate_ref, up_ref, down_ref), refs = refs[:count], refs[count : count + 3], refs[count + 3 :]
    out_refs, (lhs, wide) = refs[:count], refs[count:]
    tiles = gate_ref.shape[0] // LANES
    rows = row_refs[0].shape[0] // tiles
    for b, ref in enumerate(row_refs):
        wide[b] = ref[...].astype(F32)
        for c in range(tiles):
            lhs[b * rows : (b + 1) * rows, c * LANES : (c + 1) * LANES] = wide.at[b][
                pl.ds(c, rows, stride=tiles), :
            ].astype(BF16)
    gate_act = mm(lhs[...], gate_ref[...])
    up_act = mm(lhs[...], up_ref[...])
    act = (gate_act / (1.0 + jnp.exp(-gate_act)) * up_act).astype(BF16)
    step = 4 * LANES
    for i in range(0, down_ref.shape[1], step):
        result = mm(act, down_ref[:, i : i + step])
        for t in range(0, step, LANES):
            for b in range(count):
                wide.at[b][pl.ds((i + t) // LANES, rows, stride=tiles), :] = result[
                    b * rows : (b + 1) * rows, t : t + LANES
                ]
    for b in range(count):
        out_refs[b][...] = wide[b].astype(BF16)


def total_body(
    kept_ref, left_1_ref, right_1_ref, left_2_ref, right_2_ref, core_ref, same_ref, other_ref
):
    chips, per_expert, _ = same_ref.shape
    half = chips // 2
    first_core = jnp.broadcast_to(core_ref[...], (half, per_expert, LANES)) == 0
    for part, left_ref, right_ref in ((0, left_1_ref, right_1_ref), (1, left_2_ref, right_2_ref)):
        rows = slice(part * half, (part + 1) * half)
        sides = left_ref[...].astype(F32) + right_ref[...].astype(F32)
        result = kept_ref[rows].astype(F32) + sides
        zero, one = result[:, 0:per_expert, :], result[:, per_expert:, :]
        same_ref[rows] = jnp.where(first_core, zero, one).astype(BF16)
        other_ref[rows] = jnp.where(first_core, one, zero).astype(BF16)


def combine_body(
    experts, back_ref, normed_ref, ids_ref, weights_ref, gain_ref, bias_ref, out_ref, wide_ref, rows_ref
):
    tokens, width = normed_ref.shape
    tiles = width // LANES
    capacity = ids_ref.shape[0] * tokens // experts
    wide_ref[...] = back_ref[...].astype(F32)
    expert = lax.broadcasted_iota(jnp.int32, (experts, tokens), 0)
    weighted, rank = routing_rows(ids_ref[...], expert, weights_ref[...])
    picks = []
    for j in range(capacity):
        picks.append(jnp.where(jnp.abs(rank - j) < 0.5, weighted, 0.0))
        for c in range(tiles):
            rows_ref[j * experts : (j + 1) * experts, c * LANES : (c + 1) * LANES] = wide_ref[
                pl.ds(j * tiles + c, experts, stride=capacity * tiles), :
            ].astype(BF16)
    pick = jnp.concatenate(picks, axis=0)
    high = pick.astype(BF16)
    low = pick - high.astype(F32)
    middle = low.astype(BF16)
    last = (low - middle.astype(F32)).astype(BF16)
    rows = rows_ref[...]
    moe_sum = mm_tn(high, rows) + (mm_tn(middle, rows) + mm_tn(last, rows))
    pre_final = RESIDUAL_SCALE * normed_ref[...].astype(F32) + moe_sum
    out_ref[...] = layer_norm(pre_final, gain_ref[...], bias_ref[...]).astype(BF16)


def per_device(
    resid,
    queries,
    keys,
    values,
    doc_ids,
    sink_logits,
    out_proj,
    norm1_gain,
    norm1_bias,
    route_ids,
    route_weights,
    expert_gate,
    expert_up,
    expert_down,
    norm2_gain,
    norm2_bias,
):
    tokens = queries.shape[0]
    own, width = resid.shape
    blocks, members = lax.axis_size(SP), lax.axis_size("tp")
    experts = blocks
    capacity = route_ids.shape[1] * own // experts
    tiles = width // LANES
    packed = experts * capacity * tiles

    small = (keys.T, values.T, doc_ids.reshape(1, tokens), queries, sink_logits.reshape(1, -1))
    pack = shape((2 * HEAD_DIM + 16, WINDOW), BF16)
    core = jnp.full((1, LANES), lax.axis_index("core"), jnp.int32)
    keys_t, values_t, docs, queries, sinks, head, tail, core = call(
        functools.partial(first_body, len(small)),
        [shape(a.shape, a.dtype) for a in small] + [pack, pack, shape(core.shape, core.dtype)],
        core,
        *[in_hbm(a) for a in small],
        flops=10**5,
        specs=[VMEM] + [HBM] * len(small),
        scratch=[pltpu.SemaphoreType.DMA((len(small),))],
    )
    previous = lax.ppermute(tail, SP, [(i, i + 1) for i in range(blocks - 1)])
    following = lax.ppermute(head, SP, [(i + 1, i) for i in range(blocks - 1)])
    partial, resid = call(
        attention_body,
        [shape((tokens, width), BF16), shape(resid.shape, BF16)],
        sinks,
        queries,
        keys_t,
        values_t,
        docs,
        previous,
        following,
        in_hbm(out_proj),
        in_hbm(resid),
        flops=10**9,
        specs=[VMEM] * 7 + [HBM] * 2,
        scratch=[
            pltpu.VMEM(queries.shape, BF16),
            pltpu.VMEM(out_proj.shape, BF16),
            pltpu.SemaphoreType.DMA((2,)),
        ],
    )
    parts = lax.all_to_all(partial.reshape(members, own, width), "tp", 0, 0, tiled=True)
    normed, same, other = call(
        functools.partial(dispatch_body, experts),
        [shape((own, width), BF16)] + [shape((packed // 2, LANES), BF16)] * 2,
        parts,
        resid,
        norm1_gain.reshape(1, -1),
        norm1_bias.reshape(1, -1),
        route_ids.T,
        core,
        flops=10**9,
        scratch=[pltpu.VMEM((packed, LANES), F32)],
    )
    per_expert = capacity * tiles
    chips = experts // 2

    def exchanged(same, other):
        other = lax.ppermute(other, "core", [(0, 1), (1, 0)])
        (sent,) = call(
            pair_body,
            [shape((chips, 2 * per_expert, LANES), BF16)],
            same.reshape(chips, per_expert, LANES),
            other.reshape(chips, per_expert, LANES),
            core,
            flops=10**6,
        )
        return lax.all_to_all(sent.reshape(packed, LANES), "chip", 0, 0, tiled=True)

    arrived = exchanged(same, other)

    def turned(array, by):
        return lax.ppermute(array, "tp", [(i, (i + by) % members) for i in range(members)])

    def expert_call(*row_sets):
        count, rows = len(row_sets), row_sets[0].shape[0]
        return call(
            functools.partial(expert_body, count),
            [shape((rows, LANES), BF16)] * count,
            *row_sets,
            expert_gate[0],
            expert_up[0],
            expert_down[0],
            flops=count * rows * 10**6,
            scratch=[
                pltpu.VMEM((count * rows // tiles, width), BF16),
                pltpu.VMEM((count, rows, LANES), F32),
            ],
        )

    half = packed // 2
    first, second = arrived[:half], arrived[half:]
    left_1, right_2 = turned(first, 1), turned(second, -1)
    left_2, right_1 = turned(second, 1), turned(first, -1)
    far_1, far_2 = turned(left_1, 1), turned(right_2, -1)
    (kept,) = expert_call(arrived)
    for_left_1, for_left_2, for_right_1, for_right_2 = expert_call(left_1, left_2, right_1, right_2)
    for_far_1, for_far_2 = expert_call(far_1, far_2)
    from_right_2 = turned(for_left_2, -1)
    from_left_1 = turned(for_right_1, 1)
    for_left_1 = for_left_1.astype(F32) + turned(for_far_1, -1).astype(F32)
    for_right_2 = for_right_2.astype(F32) + turned(for_far_2, 1).astype(F32)
    from_right_1 = turned(for_left_1.astype(BF16), -1)
    from_left_2 = turned(for_right_2.astype(BF16), 1)
    sides = [from_left_1, from_right_1, from_left_2, from_right_2]
    same, other = call(
        total_body,
        [shape((chips, per_expert, LANES), BF16)] * 2,
        kept.reshape(chips, 2 * per_expert, LANES),
        *[side.reshape(chips // 2, 2 * per_expert, LANES) for side in sides],
        core,
        flops=10**7,
    )
    back = exchanged(same, other)
    (mixed,) = call(
        functools.partial(combine_body, experts),
        [shape((own, width), BF16)],
        back,
        normed,
        route_ids.T,
        route_weights.T,
        norm2_gain.reshape(1, -1),
        norm2_bias.reshape(1, -1),
        flops=10**9,
        scratch=[pltpu.VMEM((packed, LANES), F32), pltpu.VMEM((capacity * experts, width), BF16)],
    )
    return mixed


def solution(mesh):
    groups, cores = mesh.shape["grp"], 2
    chips = mesh.shape["sp"] // cores
    devices = mesh.devices.reshape(groups, chips, cores, mesh.shape["tp"])
    mesh = Mesh(devices, ("grp", *SP, "tp"))
    every = ("grp", *SP, "tp")
    group = ("grp", *SP)
    placed = (
        P(every, None),
        P(group, "tp"),
        P(group, "tp"),
        P(group, "tp"),
        P(group),
        P("tp"),
        P("tp", None),
        P(),
        P(),
        P(every, None),
        P(every, None),
        P(SP, None, "tp"),
        P(SP, None, "tp"),
        P(SP, "tp", None),
        P(),
        P(),
    )

    return jax.shard_map(
        per_device, mesh=mesh, in_specs=placed, out_specs=P(every, None), check_vma=False
    )
```

```python
import functools

import jax
import jax.numpy as jnp
from jax import lax
from jax.experimental import pallas as pl
from jax.experimental.pallas import tpu as pltpu
from jax.sharding import Mesh
from jax.sharding import PartitionSpec as P


HEAD_DIM = 64
WINDOW = 128
LANES = 128
NORM_EPSILON = 1e-05
RESIDUAL_SCALE = 1.4142135623730951
MASKED = -1e30
SP = ("chip", "core")
F32 = jnp.float32
BF16 = jnp.bfloat16


VMEM = pl.BlockSpec(memory_space=pltpu.VMEM)
HBM = pl.BlockSpec(memory_space=pltpu.HBM)


def mm(a, b):
    return jnp.dot(a, b, preferred_element_type=F32)


def mm_nt(a, b):
    return lax.dot_general(a, b, (((1,), (1,)), ((), ())), preferred_element_type=F32)


def mm_tn(a, b):
    return lax.dot_general(a, b, (((0,), (0,)), ((), ())), preferred_element_type=F32)


def call(body, out_shapes, *args, flops, specs=None, scratch=(), vmem=None):
    size = sum(a.size * a.dtype.itemsize for a in args)
    size += sum(s.size * s.dtype.itemsize for s in out_shapes)
    return pl.pallas_call(
        body,
        out_shape=out_shapes,
        in_specs=specs or [VMEM] * len(args),
        out_specs=[VMEM] * len(out_shapes),
        scratch_shapes=list(scratch),
        compiler_params=pltpu.CompilerParams(vmem_limit_bytes=vmem or 12 * 2**20),
        cost_estimate=pl.CostEstimate(flops=flops, bytes_accessed=size, transcendentals=0),
    )(*args)


def in_hbm(array):
    return pltpu.with_memory_space_constraint(array, pltpu.HBM)


def shape(dims, dtype):
    return jax.ShapeDtypeStruct(dims, dtype)


def layer_norm(values, gain, bias):
    centred = values - jnp.mean(values, -1, keepdims=True)
    variance = jnp.mean(centred * centred, -1, keepdims=True)
    return centred * lax.rsqrt(variance + NORM_EPSILON) * gain + bias


def first_body(count, core_ref, *refs):
    sources, held, (head_ref, tail_ref, core_out_ref, sems) = refs[:count], refs[count : 2 * count], refs[2 * count :]
    copies = [pltpu.make_async_copy(a, b, sems.at[i]) for i, (a, b) in enumerate(zip(sources, held))]
    for copy in copies:
        copy.start()
    core_out_ref[...] = core_ref[...]
    for copy in copies[:3]:
        copy.wait()
    keys_ref, values_ref, docs_ref = held[:3]
    tokens = keys_ref.shape[1]
    docs = docs_ref[...].astype(F32).astype(BF16)
    for ref, lo in ((head_ref, 0), (tail_ref, tokens - WINDOW)):
        cols = slice(lo, lo + WINDOW)
        ref[0:HEAD_DIM, :] = keys_ref[:, cols]
        ref[HEAD_DIM : 2 * HEAD_DIM, :] = values_ref[:, cols]
        ref[2 * HEAD_DIM :, :] = jnp.broadcast_to(docs[:, cols], (16, WINDOW))
    for copy in copies[3:]:
        copy.wait()


def attention_body(
    sink_ref,
    query_ref,
    keys_ref,
    values_ref,
    docs_ref,
    prev_ref,
    next_ref,
    proj_ref,
    member_ref,
    *refs,
):
    out_refs, att_ref = refs[:-1], refs[-1]
    tokens = query_ref.shape[0]
    heads = query_ref.shape[1] // HEAD_DIM
    own_docs = docs_ref[...].astype(F32)
    query_docs = jnp.broadcast_to(own_docs, (LANES, tokens)).T[:, 0:1]
    row = lax.broadcasted_iota(jnp.int32, (tokens, 1), 0)
    blocks = []
    for key, value, docs, first in (
        (prev_ref[0:HEAD_DIM, :], prev_ref[HEAD_DIM : 2 * HEAD_DIM, :], None, -WINDOW),
        (keys_ref[...], values_ref[...], own_docs, 0),
        (next_ref[0:HEAD_DIM, :], next_ref[HEAD_DIM : 2 * HEAD_DIM, :], None, tokens),
    ):
        if docs is None:
            ref = prev_ref if first < 0 else next_ref
            docs = ref[2 * HEAD_DIM :, :].astype(F32)[0:1, :]
        width = key.shape[1]
        place = first + lax.broadcasted_iota(jnp.int32, (1, width), 1)
        allowed = (jnp.abs(row - place) <= WINDOW) & (query_docs == docs)
        blocks.append((key, value, jnp.where(allowed, 0.0, MASKED)))
    for h in range(heads):
        cols = slice(h * HEAD_DIM, (h + 1) * HEAD_DIM)
        query = query_ref[:, cols]
        sink = sink_ref[:, h : h + 1]
        scores = [
            mm(query, key) * HEAD_DIM ** (-0.5) + hidden for key, _, hidden in blocks
        ]
        top = functools.reduce(jnp.maximum, [jnp.max(s, -1, keepdims=True) for s in scores])
        top = jnp.maximum(top, sink)
        raised = [jnp.exp(s - top) for s in scores]
        total = jnp.exp(sink - top) + sum(jnp.sum(r, -1, keepdims=True) for r in raised)
        scale = 1.0 / total
        result = sum(
            mm_nt((r * scale).astype(BF16), value) for r, (_, value, _) in zip(raised, blocks)
        )
        att_ref[:, cols] = result.astype(BF16)
    members = len(out_refs)
    own = tokens // members
    for by, out_ref in enumerate(out_refs):
        start = pl.multiple_of(lax.rem(member_ref[0] + by, members) * own, own)
        out_ref[...] = mm(att_ref[pl.ds(start, own), :], proj_ref[...]).astype(BF16)


def routing_rows(ids, expert, weights=None):
    experts, tokens = expert.shape
    named = jnp.zeros((experts, tokens), F32)
    weighted = jnp.zeros((experts, tokens), F32)
    for k in range(ids.shape[0]):
        hit = ids[k : k + 1, :] == expert
        named += hit.astype(F32)
        if weights is not None:
            weighted += jnp.where(hit, weights[k : k + 1, :], 0.0)
    before = lax.broadcasted_iota(jnp.int32, (tokens, tokens), 0) < lax.broadcasted_iota(
        jnp.int32, (tokens, tokens), 1
    )
    rank = jnp.where(named > 0.5, mm(named.astype(BF16), before.astype(BF16)), -1.0)
    return (named if weights is None else weighted), rank


def dispatch_body(experts, members, *refs):
    part_refs, (resid_ref, gain_ref, bias_ref, ids_ref, core_ref) = refs[:members], refs[members : members + 5]
    normed_ref, same_ref, other_ref, wide_ref = refs[members + 5 :]
    tokens, width = resid_ref.shape
    tiles = width // LANES
    capacity = ids_ref.shape[0] * tokens // experts
    projected = sum(ref[...].astype(F32) for ref in part_refs)
    pre_norm = RESIDUAL_SCALE * resid_ref[...].astype(F32) + projected.astype(BF16).astype(F32)
    normed = layer_norm(pre_norm, gain_ref[...], bias_ref[...]).astype(BF16)
    normed_ref[...] = normed
    chips = experts // 2
    row = lax.broadcasted_iota(jnp.int32, (experts, tokens), 0)
    core = jnp.broadcast_to(core_ref[:, 0:1], (experts, tokens))
    expert = jnp.where(row < chips, 2 * row + core, 2 * (row - chips) + 1 - core)
    named, rank = routing_rows(ids_ref[...], expert)
    for j in range(capacity):
        pick = jnp.where(jnp.abs(rank - j) < 0.5, named, 0.0).astype(BF16)
        rows = mm(pick, normed)
        for c in range(tiles):
            wide_ref[pl.ds(j * tiles + c, experts, stride=capacity * tiles), :] = rows[
                :, c * LANES : (c + 1) * LANES
            ]
    half = same_ref.shape[0]
    same_ref[...] = wide_ref[0:half, :].astype(BF16)
    other_ref[...] = wide_ref[half:, :].astype(BF16)


def pair_body(same_ref, other_ref, core_ref, out_ref):
    per_expert = same_ref.shape[1]
    first_core = jnp.broadcast_to(core_ref[...], same_ref.shape) == 0
    same, other = same_ref[...].astype(F32), other_ref[...].astype(F32)
    out_ref[:, 0:per_expert, :] = jnp.where(first_core, same, other).astype(BF16)
    out_ref[:, per_expert:, :] = jnp.where(first_core, other, same).astype(BF16)


def expert_body(count, *refs):
    row_refs, (gate_ref, up_ref, down_ref), refs = refs[:count], refs[count : count + 3], refs[count + 3 :]
    out_refs, (lhs, wide) = refs[:count], refs[count:]
    tiles = gate_ref.shape[0] // LANES
    rows = row_refs[0].shape[0] // tiles
    for b, ref in enumerate(row_refs):
        wide[b] = ref[...].astype(F32)
        for c in range(tiles):
            lhs[b * rows : (b + 1) * rows, c * LANES : (c + 1) * LANES] = wide.at[b][
                pl.ds(c, rows, stride=tiles), :
            ].astype(BF16)
    gate_act = mm(lhs[...], gate_ref[...])
    up_act = mm(lhs[...], up_ref[...])
    act = (gate_act / (1.0 + jnp.exp(-gate_act)) * up_act).astype(BF16)
    step = 4 * LANES
    for i in range(0, down_ref.shape[1], step):
        result = mm(act, down_ref[:, i : i + step])
        for t in range(0, step, LANES):
            for b in range(count):
                wide.at[b][pl.ds((i + t) // LANES, rows, stride=tiles), :] = result[
                    b * rows : (b + 1) * rows, t : t + LANES
                ]
    for b in range(count):
        out_refs[b][...] = wide[b].astype(BF16)


def total_body(
    kept_ref, left_1_ref, right_1_ref, left_2_ref, right_2_ref, core_ref, same_ref, other_ref
):
    chips, per_expert, _ = same_ref.shape
    half = chips // 2
    first_core = jnp.broadcast_to(core_ref[...], (half, per_expert, LANES)) == 0
    for part, left_ref, right_ref in ((0, left_1_ref, right_1_ref), (1, left_2_ref, right_2_ref)):
        rows = slice(part * half, (part + 1) * half)
        sides = left_ref[...].astype(F32) + right_ref[...].astype(F32)
        result = kept_ref[rows].astype(F32) + sides
        zero, one = result[:, 0:per_expert, :], result[:, per_expert:, :]
        same_ref[rows] = jnp.where(first_core, zero, one).astype(BF16)
        other_ref[rows] = jnp.where(first_core, one, zero).astype(BF16)


def combine_body(
    experts, back_ref, normed_ref, ids_ref, weights_ref, gain_ref, bias_ref, out_ref, wide_ref, rows_ref
):
    tokens, width = normed_ref.shape
    tiles = width // LANES
    capacity = ids_ref.shape[0] * tokens // experts
    wide_ref[...] = back_ref[...].astype(F32)
    expert = lax.broadcasted_iota(jnp.int32, (experts, tokens), 0)
    weighted, rank = routing_rows(ids_ref[...], expert, weights_ref[...])
    picks = []
    for j in range(capacity):
        picks.append(jnp.where(jnp.abs(rank - j) < 0.5, weighted, 0.0))
        for c in range(tiles):
            rows_ref[j * experts : (j + 1) * experts, c * LANES : (c + 1) * LANES] = wide_ref[
                pl.ds(j * tiles + c, experts, stride=capacity * tiles), :
            ].astype(BF16)
    pick = jnp.concatenate(picks, axis=0)
    high = pick.astype(BF16)
    low = pick - high.astype(F32)
    middle = low.astype(BF16)
    last = (low - middle.astype(F32)).astype(BF16)
    rows = rows_ref[...]
    moe_sum = mm_tn(high, rows) + (mm_tn(middle, rows) + mm_tn(last, rows))
    pre_final = RESIDUAL_SCALE * normed_ref[...].astype(F32) + moe_sum
    out_ref[...] = layer_norm(pre_final, gain_ref[...], bias_ref[...]).astype(BF16)


def per_device(
    resid,
    queries,
    keys,
    values,
    doc_ids,
    sink_logits,
    out_proj,
    norm1_gain,
    norm1_bias,
    route_ids,
    route_weights,
    expert_gate,
    expert_up,
    expert_down,
    norm2_gain,
    norm2_bias,
):
    tokens = queries.shape[0]
    own, width = resid.shape
    blocks, members = lax.axis_size(SP), lax.axis_size("tp")
    experts = blocks
    capacity = route_ids.shape[1] * own // experts
    tiles = width // LANES
    packed = experts * capacity * tiles

    small = (keys.T, values.T, doc_ids.reshape(1, tokens), queries, out_proj, resid, sink_logits.reshape(1, -1))
    pack = shape((2 * HEAD_DIM + 16, WINDOW), BF16)
    core = jnp.full((1, LANES), lax.axis_index("core"), jnp.int32)
    keys_t, values_t, docs, queries, out_proj, resid, sinks, head, tail, core = call(
        functools.partial(first_body, len(small)),
        [shape(a.shape, a.dtype) for a in small] + [pack, pack, shape(core.shape, core.dtype)],
        core,
        *[in_hbm(a) for a in small],
        flops=10**5,
        specs=[VMEM] + [HBM] * len(small),
        scratch=[pltpu.SemaphoreType.DMA((len(small),))],
    )
    previous = lax.ppermute(tail, SP, [(i, (i + 1) % blocks) for i in range(blocks)])
    following = lax.ppermute(head, SP, [((i + 1) % blocks, i) for i in range(blocks)])
    shares = call(
        attention_body,
        [shape((own, width), BF16)] * members,
        sinks,
        queries,
        keys_t,
        values_t,
        docs,
        previous,
        following,
        out_proj,
        lax.axis_index("tp").astype(jnp.int32).reshape(1),
        flops=10**9,
        specs=[VMEM] * 8 + [pl.BlockSpec(memory_space=pltpu.SMEM)],
        scratch=[pltpu.VMEM(queries.shape, BF16)],
    )

    def turned(array, by):
        return lax.ppermute(array, "tp", [(i, (i + by) % members) for i in range(members)])

    parts = [shares[0]] + [turned(shares[by], by) for by in range(1, members)]
    normed, same, other = call(
        functools.partial(dispatch_body, experts, members),
        [shape((own, width), BF16)] + [shape((packed // 2, LANES), BF16)] * 2,
        *parts,
        resid,
        norm1_gain.reshape(1, -1),
        norm1_bias.reshape(1, -1),
        route_ids.T,
        core,
        flops=10**9,
        scratch=[pltpu.VMEM((packed, LANES), F32)],
    )
    per_expert = capacity * tiles
    chips = experts // 2

    def exchanged(same, other):
        other = lax.ppermute(other, "core", [(0, 1), (1, 0)])
        (sent,) = call(
            pair_body,
            [shape((chips, 2 * per_expert, LANES), BF16)],
            same.reshape(chips, per_expert, LANES),
            other.reshape(chips, per_expert, LANES),
            core,
            flops=10**6,
        )
        return lax.all_to_all(sent.reshape(packed, LANES), "chip", 0, 0, tiled=True)

    arrived = exchanged(same, other)

    def expert_call(*row_sets):
        count, rows = len(row_sets), row_sets[0].shape[0]
        return call(
            functools.partial(expert_body, count),
            [shape((rows, LANES), BF16)] * count,
            *row_sets,
            expert_gate[0],
            expert_up[0],
            expert_down[0],
            flops=count * rows * 10**6,
            scratch=[
                pltpu.VMEM((count * rows // tiles, width), BF16),
                pltpu.VMEM((count, rows, LANES), F32),
            ],
        )

    half = packed // 2
    first, second = arrived[:half], arrived[half:]
    left_1, right_2 = turned(first, 1), turned(second, -1)
    left_2, right_1 = turned(second, 1), turned(first, -1)
    far_1, far_2 = turned(left_1, 1), turned(right_2, -1)
    (kept,) = expert_call(arrived)
    for_left_1, for_left_2, for_right_1, for_right_2 = expert_call(left_1, left_2, right_1, right_2)
    for_far_1, for_far_2 = expert_call(far_1, far_2)
    from_right_2 = turned(for_left_2, -1)
    from_left_1 = turned(for_right_1, 1)
    for_left_1 = for_left_1.astype(F32) + turned(for_far_1, -1).astype(F32)
    for_right_2 = for_right_2.astype(F32) + turned(for_far_2, 1).astype(F32)
    from_right_1 = turned(for_left_1.astype(BF16), -1)
    from_left_2 = turned(for_right_2.astype(BF16), 1)
    sides = [from_left_1, from_right_1, from_left_2, from_right_2]
    same, other = call(
        total_body,
        [shape((chips, per_expert, LANES), BF16)] * 2,
        kept.reshape(chips, 2 * per_expert, LANES),
        *[side.reshape(chips // 2, 2 * per_expert, LANES) for side in sides],
        core,
        flops=10**7,
    )
    back = exchanged(same, other)
    (mixed,) = call(
        functools.partial(combine_body, experts),
        [shape((own, width), BF16)],
        back,
        normed,
        route_ids.T,
        route_weights.T,
        norm2_gain.reshape(1, -1),
        norm2_bias.reshape(1, -1),
        flops=10**9,
        scratch=[pltpu.VMEM((packed, LANES), F32), pltpu.VMEM((capacity * experts, width), BF16)],
    )
    return mixed


def solution(mesh):
    groups, cores = mesh.shape["grp"], 2
    chips = mesh.shape["sp"] // cores
    devices = mesh.devices.reshape(groups, chips, cores, mesh.shape["tp"])
    mesh = Mesh(devices, ("grp", *SP, "tp"))
    every = ("grp", *SP, "tp")
    group = ("grp", *SP)
    placed = (
        P(every, None),
        P(group, "tp"),
        P(group, "tp"),
        P(group, "tp"),
        P(group),
        P("tp"),
        P("tp", None),
        P(),
        P(),
        P(every, None),
        P(every, None),
        P(SP, None, "tp"),
        P(SP, None, "tp"),
        P(SP, "tp", None),
        P(),
        P(),
    )

    return jax.shard_map(per_device, mesh=mesh, in_specs=placed, out_specs=P(every, None), check_vma=False)
```

```python
import functools

import jax
import jax.numpy as jnp
from jax import lax
from jax.experimental import pallas as pl
from jax.experimental.pallas import tpu as pltpu
from jax.sharding import Mesh
from jax.sharding import PartitionSpec as P


HEAD_DIM = 64
WINDOW = 128
LANES = 128
NORM_EPSILON = 1e-05
RESIDUAL_SCALE = 1.4142135623730951
MASKED = -1e30
SP = ("chip", "core")
F32 = jnp.float32
BF16 = jnp.bfloat16


VMEM = pl.BlockSpec(memory_space=pltpu.VMEM)
HBM = pl.BlockSpec(memory_space=pltpu.HBM)


def mm(a, b):
    return jnp.dot(a, b, preferred_element_type=F32)


def mm_nt(a, b):
    return lax.dot_general(a, b, (((1,), (1,)), ((), ())), preferred_element_type=F32)


def mm_tn(a, b):
    return lax.dot_general(a, b, (((0,), (0,)), ((), ())), preferred_element_type=F32)


def call(body, out_shapes, *args, flops, specs=None, scratch=(), vmem=None):
    size = sum(a.size * a.dtype.itemsize for a in args)
    size += sum(s.size * s.dtype.itemsize for s in out_shapes)
    return pl.pallas_call(
        body,
        out_shape=out_shapes,
        in_specs=specs or [VMEM] * len(args),
        out_specs=[VMEM] * len(out_shapes),
        scratch_shapes=list(scratch),
        compiler_params=pltpu.CompilerParams(vmem_limit_bytes=vmem or 12 * 2**20),
        cost_estimate=pl.CostEstimate(flops=flops, bytes_accessed=size, transcendentals=0),
    )(*args)


def in_hbm(array):
    return pltpu.with_memory_space_constraint(array, pltpu.HBM)


def shape(dims, dtype):
    return jax.ShapeDtypeStruct(dims, dtype)


def layer_norm(values, gain, bias):
    centred = values - jnp.mean(values, -1, keepdims=True)
    variance = jnp.mean(centred * centred, -1, keepdims=True)
    return centred * lax.rsqrt(variance + NORM_EPSILON) * gain + bias


def first_body(count, core_ref, *refs):
    sources, held, (head_ref, tail_ref, core_out_ref, sems) = refs[:count], refs[count : 2 * count], refs[2 * count :]
    copies = [pltpu.make_async_copy(a, b, sems.at[i]) for i, (a, b) in enumerate(zip(sources, held))]
    for copy in copies:
        copy.start()
    core_out_ref[...] = core_ref[...]
    for copy in copies[:3]:
        copy.wait()
    keys_ref, values_ref, docs_ref = held[:3]
    tokens = keys_ref.shape[1]
    docs = docs_ref[...].astype(F32).astype(BF16)
    for ref, lo in ((head_ref, 0), (tail_ref, tokens - WINDOW)):
        cols = slice(lo, lo + WINDOW)
        ref[0:HEAD_DIM, :] = keys_ref[:, cols]
        ref[HEAD_DIM : 2 * HEAD_DIM, :] = values_ref[:, cols]
        ref[2 * HEAD_DIM :, :] = jnp.broadcast_to(docs[:, cols], (16, WINDOW))
    for copy in copies[3:]:
        copy.wait()


def fetch_body(count, *refs):
    sources, held, sems = refs[:count], refs[count : 2 * count], refs[2 * count]
    copies = [pltpu.make_async_copy(a, b, sems.at[i]) for i, (a, b) in enumerate(zip(sources, held))]
    for copy in copies:
        copy.start()
    for copy in copies:
        copy.wait()


def attention_body(
    sink_ref,
    query_ref,
    keys_ref,
    values_ref,
    docs_ref,
    prev_ref,
    next_ref,
    proj_ref,
    member_ref,
    *refs,
):
    out_refs, att_ref = refs[:-1], refs[-1]
    tokens = query_ref.shape[0]
    heads = query_ref.shape[1] // HEAD_DIM
    own_docs = docs_ref[...].astype(F32)
    query_docs = jnp.broadcast_to(own_docs, (LANES, tokens)).T[:, 0:1]
    row = lax.broadcasted_iota(jnp.int32, (tokens, 1), 0)
    blocks = []
    for key, value, docs, first in (
        (prev_ref[0:HEAD_DIM, :], prev_ref[HEAD_DIM : 2 * HEAD_DIM, :], None, -WINDOW),
        (keys_ref[...], values_ref[...], own_docs, 0),
        (next_ref[0:HEAD_DIM, :], next_ref[HEAD_DIM : 2 * HEAD_DIM, :], None, tokens),
    ):
        if docs is None:
            ref = prev_ref if first < 0 else next_ref
            docs = ref[2 * HEAD_DIM :, :].astype(F32)[0:1, :]
        width = key.shape[1]
        place = first + lax.broadcasted_iota(jnp.int32, (1, width), 1)
        allowed = (jnp.abs(row - place) <= WINDOW) & (query_docs == docs)
        blocks.append((key, value, jnp.where(allowed, 0.0, MASKED)))
    for h in range(heads):
        cols = slice(h * HEAD_DIM, (h + 1) * HEAD_DIM)
        query = query_ref[:, cols]
        sink = sink_ref[:, h : h + 1]
        scores = [
            mm(query, key) * HEAD_DIM ** (-0.5) + hidden for key, _, hidden in blocks
        ]
        top = functools.reduce(jnp.maximum, [jnp.max(s, -1, keepdims=True) for s in scores])
        top = jnp.maximum(top, sink)
        raised = [jnp.exp(s - top) for s in scores]
        total = jnp.exp(sink - top) + sum(jnp.sum(r, -1, keepdims=True) for r in raised)
        scale = 1.0 / total
        result = sum(
            mm_nt((r * scale).astype(BF16), value) for r, (_, value, _) in zip(raised, blocks)
        )
        att_ref[:, cols] = result.astype(BF16)
    members = len(out_refs)
    own = tokens // members
    ordered = []
    for by in range(members):
        start = pl.multiple_of(lax.rem(member_ref[0] + by, members) * own, own)
        ordered.append(att_ref[pl.ds(start, own), :])
    shares = mm(jnp.concatenate(ordered, axis=0), proj_ref[...])
    for by, out_ref in enumerate(out_refs):
        out_ref[...] = shares[by * own : (by + 1) * own].astype(BF16)


def routing_rows(ids, expert, weights=None):
    experts, tokens = expert.shape
    named = jnp.zeros((experts, tokens), F32)
    weighted = jnp.zeros((experts, tokens), F32)
    for k in range(ids.shape[0]):
        hit = ids[k : k + 1, :] == expert
        named += hit.astype(F32)
        if weights is not None:
            weighted += jnp.where(hit, weights[k : k + 1, :], 0.0)
    before = lax.broadcasted_iota(jnp.int32, (tokens, tokens), 0) < lax.broadcasted_iota(
        jnp.int32, (tokens, tokens), 1
    )
    rank = jnp.where(named > 0.5, mm(named.astype(BF16), before.astype(BF16)), -1.0)
    return (named if weights is None else weighted), rank


def dispatch_body(experts, members, *refs):
    part_refs, (resid_ref, gain_ref, bias_ref, ids_ref, core_ref) = refs[:members], refs[members : members + 5]
    normed_ref, same_ref, other_ref, wide_ref = refs[members + 5 :]
    tokens, width = resid_ref.shape
    tiles = width // LANES
    capacity = ids_ref.shape[0] * tokens // experts
    projected = sum(ref[...].astype(F32) for ref in part_refs)
    pre_norm = RESIDUAL_SCALE * resid_ref[...].astype(F32) + projected.astype(BF16).astype(F32)
    normed = layer_norm(pre_norm, gain_ref[...], bias_ref[...]).astype(BF16)
    normed_ref[...] = normed
    chips = experts // 2
    row = lax.broadcasted_iota(jnp.int32, (experts, tokens), 0)
    core = jnp.broadcast_to(core_ref[:, 0:1], (experts, tokens))
    expert = jnp.where(row < chips, 2 * row + core, 2 * (row - chips) + 1 - core)
    named, rank = routing_rows(ids_ref[...], expert)
    for j in range(capacity):
        pick = jnp.where(jnp.abs(rank - j) < 0.5, named, 0.0).astype(BF16)
        rows = mm(pick, normed)
        for c in range(tiles):
            wide_ref[pl.ds(j * tiles + c, experts, stride=capacity * tiles), :] = rows[
                :, c * LANES : (c + 1) * LANES
            ]
    half = same_ref.shape[0]
    same_ref[...] = wide_ref[0:half, :].astype(BF16)
    other_ref[...] = wide_ref[half:, :].astype(BF16)


def pair_body(same_ref, other_ref, core_ref, out_ref):
    per_expert = same_ref.shape[1]
    first_core = jnp.broadcast_to(core_ref[...], same_ref.shape) == 0
    same, other = same_ref[...].astype(F32), other_ref[...].astype(F32)
    out_ref[:, 0:per_expert, :] = jnp.where(first_core, same, other).astype(BF16)
    out_ref[:, per_expert:, :] = jnp.where(first_core, other, same).astype(BF16)


def expert_body(count, *refs):
    row_refs, (gate_ref, up_ref, down_ref), refs = refs[:count], refs[count : count + 3], refs[count + 3 :]
    out_refs, (lhs, wide) = refs[:count], refs[count:]
    tiles = gate_ref.shape[0] // LANES
    rows = row_refs[0].shape[0] // tiles
    for b, ref in enumerate(row_refs):
        wide[b] = ref[...].astype(F32)
        for c in range(tiles):
            lhs[b * rows : (b + 1) * rows, c * LANES : (c + 1) * LANES] = wide.at[b][
                pl.ds(c, rows, stride=tiles), :
            ].astype(BF16)
    gate_act = mm(lhs[...], gate_ref[...])
    up_act = mm(lhs[...], up_ref[...])
    act = (gate_act / (1.0 + jnp.exp(-gate_act)) * up_act).astype(BF16)
    step = 4 * LANES
    for i in range(0, down_ref.shape[1], step):
        result = mm(act, down_ref[:, i : i + step])
        for t in range(0, step, LANES):
            for b in range(count):
                wide.at[b][pl.ds((i + t) // LANES, rows, stride=tiles), :] = result[
                    b * rows : (b + 1) * rows, t : t + LANES
                ]
    for b in range(count):
        out_refs[b][...] = wide[b].astype(BF16)


def total_body(
    kept_ref, left_1_ref, right_1_ref, left_2_ref, right_2_ref, core_ref, same_ref, other_ref
):
    chips, per_expert, _ = same_ref.shape
    half = chips // 2
    first_core = jnp.broadcast_to(core_ref[...], (half, per_expert, LANES)) == 0
    for part, left_ref, right_ref in ((0, left_1_ref, right_1_ref), (1, left_2_ref, right_2_ref)):
        rows = slice(part * half, (part + 1) * half)
        sides = left_ref[...].astype(F32) + right_ref[...].astype(F32)
        result = kept_ref[rows].astype(F32) + sides
        zero, one = result[:, 0:per_expert, :], result[:, per_expert:, :]
        same_ref[rows] = jnp.where(first_core, zero, one).astype(BF16)
        other_ref[rows] = jnp.where(first_core, one, zero).astype(BF16)


def combine_body(
    experts, back_ref, normed_ref, ids_ref, weights_ref, gain_ref, bias_ref, out_ref, wide_ref, rows_ref
):
    tokens, width = normed_ref.shape
    tiles = width // LANES
    capacity = ids_ref.shape[0] * tokens // experts
    wide_ref[...] = back_ref[...].astype(F32)
    expert = lax.broadcasted_iota(jnp.int32, (experts, tokens), 0)
    weighted, rank = routing_rows(ids_ref[...], expert, weights_ref[...])
    picks = []
    for j in range(capacity):
        picks.append(jnp.where(jnp.abs(rank - j) < 0.5, weighted, 0.0))
        for c in range(tiles):
            rows_ref[j * experts : (j + 1) * experts, c * LANES : (c + 1) * LANES] = wide_ref[
                pl.ds(j * tiles + c, experts, stride=capacity * tiles), :
            ].astype(BF16)
    pick = jnp.concatenate(picks, axis=0)
    high = pick.astype(BF16)
    low = pick - high.astype(F32)
    middle = low.astype(BF16)
    last = (low - middle.astype(F32)).astype(BF16)
    rows = rows_ref[...]
    moe_sum = mm_tn(high, rows) + (mm_tn(middle, rows) + mm_tn(last, rows))
    pre_final = RESIDUAL_SCALE * normed_ref[...].astype(F32) + moe_sum
    out_ref[...] = layer_norm(pre_final, gain_ref[...], bias_ref[...]).astype(BF16)


def per_device(
    resid,
    queries,
    keys,
    values,
    doc_ids,
    sink_logits,
    out_proj,
    norm1_gain,
    norm1_bias,
    route_ids,
    route_weights,
    expert_gate,
    expert_up,
    expert_down,
    norm2_gain,
    norm2_bias,
):
    tokens = queries.shape[0]
    own, width = resid.shape
    blocks, members = lax.axis_size(SP), lax.axis_size("tp")
    experts = blocks
    capacity = route_ids.shape[1] * own // experts
    tiles = width // LANES
    packed = experts * capacity * tiles

    small = (keys.T, values.T, doc_ids.reshape(1, tokens), queries, sink_logits.reshape(1, -1))
    pack = shape((2 * HEAD_DIM + 16, WINDOW), BF16)
    core = jnp.full((1, LANES), lax.axis_index("core"), jnp.int32)
    keys_t, values_t, docs, queries, sinks, head, tail, core = call(
        functools.partial(first_body, len(small)),
        [shape(a.shape, a.dtype) for a in small] + [pack, pack, shape(core.shape, core.dtype)],
        core,
        *[in_hbm(a) for a in small],
        flops=10**5,
        specs=[VMEM] + [HBM] * len(small),
        scratch=[pltpu.SemaphoreType.DMA((len(small),))],
    )
    previous = lax.ppermute(tail, SP, [(i, (i + 1) % blocks) for i in range(blocks)])
    following = lax.ppermute(head, SP, [((i + 1) % blocks, i) for i in range(blocks)])
    later = (out_proj, resid)
    out_proj, resid = call(
        functools.partial(fetch_body, len(later)),
        [shape(a.shape, a.dtype) for a in later],
        *[in_hbm(a) for a in later],
        flops=10**5,
        specs=[HBM] * len(later),
        scratch=[pltpu.SemaphoreType.DMA((len(later),))],
    )
    shares = call(
        attention_body,
        [shape((own, width), BF16)] * members,
        sinks,
        queries,
        keys_t,
        values_t,
        docs,
        previous,
        following,
        out_proj,
        lax.axis_index("tp").astype(jnp.int32).reshape(1),
        flops=10**9,
        specs=[VMEM] * 8 + [pl.BlockSpec(memory_space=pltpu.SMEM)],
        scratch=[pltpu.VMEM(queries.shape, BF16)],
    )

    def turned(array, by):
        return lax.ppermute(array, "tp", [(i, (i + by) % members) for i in range(members)])

    parts = [shares[0]] + [turned(shares[by], by) for by in range(1, members)]
    normed, same, other = call(
        functools.partial(dispatch_body, experts, members),
        [shape((own, width), BF16)] + [shape((packed // 2, LANES), BF16)] * 2,
        *parts,
        resid,
        norm1_gain.reshape(1, -1),
        norm1_bias.reshape(1, -1),
        route_ids.T,
        core,
        flops=10**9,
        scratch=[pltpu.VMEM((packed, LANES), F32)],
    )
    per_expert = capacity * tiles
    chips = experts // 2

    def exchanged(same, other):
        other = lax.ppermute(other, "core", [(0, 1), (1, 0)])
        (sent,) = call(
            pair_body,
            [shape((chips, 2 * per_expert, LANES), BF16)],
            same.reshape(chips, per_expert, LANES),
            other.reshape(chips, per_expert, LANES),
            core,
            flops=10**6,
        )
        return lax.all_to_all(sent.reshape(packed, LANES), "chip", 0, 0, tiled=True)

    arrived = exchanged(same, other)

    def expert_call(*row_sets):
        count, rows = len(row_sets), row_sets[0].shape[0]
        return call(
            functools.partial(expert_body, count),
            [shape((rows, LANES), BF16)] * count,
            *row_sets,
            expert_gate[0],
            expert_up[0],
            expert_down[0],
            flops=count * rows * 10**6,
            scratch=[
                pltpu.VMEM((count * rows // tiles, width), BF16),
                pltpu.VMEM((count, rows, LANES), F32),
            ],
        )

    half = packed // 2
    first, second = arrived[:half], arrived[half:]
    left_1, right_2 = turned(first, 1), turned(second, -1)
    left_2, right_1 = turned(second, 1), turned(first, -1)
    far_1, far_2 = turned(left_1, 1), turned(right_2, -1)
    (kept,) = expert_call(arrived)
    for_left_1, for_left_2, for_right_1, for_right_2 = expert_call(left_1, left_2, right_1, right_2)
    for_far_1, for_far_2 = expert_call(far_1, far_2)
    from_right_2 = turned(for_left_2, -1)
    from_left_1 = turned(for_right_1, 1)
    for_left_1 = for_left_1.astype(F32) + turned(for_far_1, -1).astype(F32)
    for_right_2 = for_right_2.astype(F32) + turned(for_far_2, 1).astype(F32)
    from_right_1 = turned(for_left_1.astype(BF16), -1)
    from_left_2 = turned(for_right_2.astype(BF16), 1)
    sides = [from_left_1, from_right_1, from_left_2, from_right_2]
    same, other = call(
        total_body,
        [shape((chips, per_expert, LANES), BF16)] * 2,
        kept.reshape(chips, 2 * per_expert, LANES),
        *[side.reshape(chips // 2, 2 * per_expert, LANES) for side in sides],
        core,
        flops=10**7,
    )
    back = exchanged(same, other)
    (mixed,) = call(
        functools.partial(combine_body, experts),
        [shape((own, width), BF16)],
        back,
        normed,
        route_ids.T,
        route_weights.T,
        norm2_gain.reshape(1, -1),
        norm2_bias.reshape(1, -1),
        flops=10**9,
        scratch=[pltpu.VMEM((packed, LANES), F32), pltpu.VMEM((capacity * experts, width), BF16)],
    )
    return mixed


def solution(mesh):
    groups, cores = mesh.shape["grp"], 2
    chips = mesh.shape["sp"] // cores
    devices = mesh.devices.reshape(groups, chips, cores, mesh.shape["tp"])
    mesh = Mesh(devices, ("grp", *SP, "tp"))
    every = ("grp", *SP, "tp")
    group = ("grp", *SP)
    placed = (
        P(every, None),
        P(group, "tp"),
        P(group, "tp"),
        P(group, "tp"),
        P(group),
        P("tp"),
        P("tp", None),
        P(),
        P(),
        P(every, None),
        P(every, None),
        P(SP, None, "tp"),
        P(SP, None, "tp"),
        P(SP, "tp", None),
        P(),
        P(),
    )

    return jax.shard_map(per_device, mesh=mesh, in_specs=placed, out_specs=P(every, None), check_vma=False)
```
